32 devices in a mesh: fs: 8 (over z, x), tp: 4 (over y, core).
Axes of the slice: x: 2, y: 2, z: 4, core: 2. Of those that a mesh axis runs over, the one named last changes fastest.
Arguments:
- tokens: bfloat16 [2048, 3072], P('tp', 'fs'), may hold values from -6 to 6
- mix_gain: float32 [2048], replicated, may hold values from 0.1 to 1.9
- mlp_gain: float32 [2048], replicated, may hold values from 0.1 to 1.9
- query_weight: float32 [2048, 1024], P('fs', 'tp'), may hold values from -0.125 to 0.125
- key_weight: float32 [2048, 1024], P('fs', 'tp'), may hold values from -0.125 to 0.125
- value_weight: float32 [2048, 1024], P('fs', 'tp'), may hold values from -0.125 to 0.125
- gate_weight: float32 [2048, 1024], P('fs', 'tp'), may hold values from -0.125 to 0.125
- out_weight: float32 [1024, 2048], P('tp', 'fs'), may hold values from -0.1875 to 0.1875
- up_weight: float32 [2048, 8192], P('fs', 'tp'), may hold values from -0.125 to 0.125
- down_weight: float32 [8192, 2048], P('tp', 'fs'), may hold values from -0.0625 to 0.0625
- query_scale: float32 [1024], P(('tp', 'fs')), may hold values from 0.1 to 1.9
- key_scale: float32 [1024], P(('tp', 'fs')), may hold values from 0.1 to 1.9
- value_scale: float32 [1024], P(('tp', 'fs')), may hold values from 0.1 to 1.9
- gate_scale: float32 [1024], P(('tp', 'fs')), may hold values from 0.1 to 1.9
- out_scale: float32 [2048], P(('tp', 'fs')), may hold values from 0.1 to 1.9
- up_scale: float32 [8192], P(('tp', 'fs')), may hold values from 0.1 to 1.9
- down_scale: float32 [2048], P(('tp', 'fs')), may hold values from 0.1 to 1.9
- forget: float32 [16], P('tp'), as said below
Outputs:
- layer_out: bfloat16 [2048, 3072], P('tp', 'fs')
The draws below stay inside these ranges and needn't reach their ends.
Inputs may be any that keep to these rules, and one draw needn't show every extreme that they name: `forget`: positive rates; each head either forgets within a few tens of positions or keeps a tenth or more over a whole sequence of 384.
All inputs are finite; a program needn't handle non-finite values.
Results may differ from the reference program's by a relative error of at most 0.02.
Values may be sent and summed in bfloat16 or wider, within the bound.
A program may use at most 64 MiB of HBM per device.

```python
import math
import jax
import jax.numpy as jnp
from jax import lax

D = 2048
HEADS = 16
HEAD_DIM = 64
FF = 8192
LEN = 384
RET_W = 1024
TOKENS = 3072
N_FS = 8
N_TP = 4


def draw_forget(key, part):
    first, second, third = jax.random.split(key, 3)
    fast = jax.random.randint(first, (HEADS,), 0, 16) < 8
    quick = jax.random.uniform(second, (HEADS,), jnp.float32, 1.0 / 50.0, 1.0 / 25.0)
    slow = jnp.exp(jax.random.uniform(third, (HEADS,), jnp.float32, math.log(0.1 / LEN), math.log(2.0 / LEN)))
    return jnp.where(fast, quick, slow).astype(jnp.float32)


def shard_levels(key, dims, cuts, smallest, largest):
    factor_of, own = 1.0, jax.random.fold_in(key, 6)
    for dim, shards_of in cuts:
        draws = jnp.exp(jax.random.uniform(jax.random.fold_in(own, dim), (shards_of,), jnp.float32, smallest / len(cuts), largest / len(cuts)))
        factor_of = factor_of * jnp.repeat(draws, dims[dim] // shards_of).reshape([-1 if axis == dim else 1 for axis in range(len(dims))])
    return factor_of


def centred(rng, extent, deviation, limit, cuts=(), held_as=jnp.bfloat16):
    array = deviation * jax.random.normal(rng, extent, jnp.float32)
    if cuts:
        array = array * shard_levels(rng, extent, cuts, -0.22, 0.18)
    return jnp.clip(array, -limit, limit).astype(held_as)


def setup_inputs(seed: int = 0) -> dict:
    key_list = jax.random.split(jax.random.key(seed), 19)
    tokens = centred(key_list[0], (D, TOKENS), 1.0, 6.0, ((0, 4), (1, 8)))
    mix_gain = jnp.clip(1.0 + 0.18 * jax.random.normal(key_list[1], (D,), jnp.float32), 0.1, 1.9)
    mlp_gain = jnp.clip(1.0 + 0.18 * jax.random.normal(key_list[2], (D,), jnp.float32), 0.1, 1.9)
    query_weight = centred(key_list[3], (D, RET_W), D ** -0.5, 0.125, ((0, 8), (1, 4)), jnp.float32)
    key_weight = centred(key_list[4], (D, RET_W), D ** -0.5, 0.125, ((0, 8), (1, 4)), jnp.float32)
    value_weight = centred(key_list[5], (D, RET_W), D ** -0.5, 0.125, ((0, 8), (1, 4)), jnp.float32)
    gate_weight = centred(key_list[6], (D, RET_W), D ** -0.5, 0.125, ((0, 8), (1, 4)), jnp.float32)
    out_weight = centred(key_list[7], (RET_W, D), RET_W ** -0.5, 0.1875, ((0, 4), (1, 8)), jnp.float32)
    up_weight = centred(key_list[8], (D, FF), D ** -0.5, 0.125, ((0, 8), (1, 4)), jnp.float32)
    down_weight = centred(key_list[9], (FF, D), FF ** -0.5, 0.0625, ((0, 4), (1, 8)), jnp.float32)
    query_scale = jnp.clip(1.0 + 0.18 * jax.random.normal(key_list[10], (RET_W,), jnp.float32), 0.1, 1.9)
    key_scale = jnp.clip(1.0 + 0.18 * jax.random.normal(key_list[11], (RET_W,), jnp.float32), 0.1, 1.9)
    value_scale = jnp.clip(1.0 + 0.18 * jax.random.normal(key_list[12], (RET_W,), jnp.float32), 0.1, 1.9)
    gate_scale = jnp.clip(1.0 + 0.18 * jax.random.normal(key_list[13], (RET_W,), jnp.float32), 0.1, 1.9)
    out_scale = jnp.clip(1.0 + 0.18 * jax.random.normal(key_list[14], (D,), jnp.float32), 0.1, 1.9)
    up_scale = jnp.clip(1.0 + 0.18 * jax.random.normal(key_list[15], (FF,), jnp.float32), 0.1, 1.9)
    down_scale = jnp.clip(1.0 + 0.18 * jax.random.normal(key_list[16], (D,), jnp.float32), 0.1, 1.9)
    forget = draw_forget(jax.random.fold_in(key_list[18], 71), 0)
    return dict(tokens=tokens, mix_gain=mix_gain, mlp_gain=mlp_gain, query_weight=query_weight, key_weight=key_weight, value_weight=value_weight, gate_weight=gate_weight, out_weight=out_weight, up_weight=up_weight, down_weight=down_weight, query_scale=query_scale, key_scale=key_scale, value_scale=value_scale, gate_scale=gate_scale, out_scale=out_scale, up_scale=up_scale, down_scale=down_scale, forget=forget)


def rotary(field, pos):
    half = field.shape[-1] // 2
    inverse = 1.0 / 10000.0 ** jnp.linspace(0.0, 1.0, half, dtype=jnp.float32)
    angle = pos[:, None] * inverse[None, :]
    cosine = jnp.cos(angle)[None, :, None, :]
    sine = jnp.sin(angle)[None, :, None, :]
    paired = field.astype(jnp.float32).reshape(field.shape[:-1] + (half, 2))
    first, second = (paired[..., 0], paired[..., 1])
    turned = jnp.stack([first * cosine - second * sine, first * sine + second * cosine], axis=-1)
    return turned.reshape(field.shape)

def retain(query, key, value, gate, forget):
    batch, length, heads, width = query.shape
    block = 128
    count = length // block
    top = lax.Precision.HIGHEST
    pos = jnp.arange(length, dtype=jnp.float32)
    rot_q = rotary(query, pos)
    rot_k = rotary(key, pos) * width ** (-0.5)
    vals = value.astype(jnp.float32)
    log_decay = -forget.astype(jnp.float32)
    steps = jnp.arange(block, dtype=jnp.float32)
    offset = steps[:, None] - steps[None, :]
    decay_mask = jnp.where(offset >= 0, jnp.exp(log_decay[:, None, None] * jnp.maximum(offset, 0.0)), 0.0)
    q_blocks = rot_q.reshape(batch, count, block, heads, width)
    k_blocks = rot_k.reshape(batch, count, block, heads, width)
    v_blocks = vals.reshape(batch, count, block, heads, width)
    inner = jnp.einsum('bnihd,bnjhd->bnhij', q_blocks, k_blocks, precision=top) * decay_mask
    inner = jnp.einsum('bnhij,bnjhe->bnihe', inner, v_blocks, precision=top)
    tail = jnp.exp(log_decay[:, None] * (block - 1.0 - steps)[None, :])
    update = jnp.einsum('bnjhd,bnjhe,hj->nbhde', k_blocks, v_blocks, tail, precision=top)
    block_decay = jnp.exp(log_decay * block)[None, :, None, None]

    def advance(state, piece):
        return (state * block_decay + piece, state)
    start_state = jnp.zeros((batch, heads, width, width), jnp.float32)
    _, before = lax.scan(advance, start_state, update)
    lead = jnp.exp(log_decay[None, :] * (steps[:, None] + 1.0))
    cross = jnp.einsum('bnihd,nbhde->bnihe', q_blocks, before, precision=top) * lead[None, None, :, :, None]
    total = inner + cross
    total = total * lax.rsqrt(lax.optimization_barrier(jnp.mean(total * total, axis=-1, keepdims=True)) + 0.01)
    total = total.reshape(batch, length, heads, width)
    return jax.nn.silu(gate.astype(jnp.float32)) * total

def norm_rows(rows, gain):
    scale = lax.rsqrt(lax.optimization_barrier(jnp.mean(rows * rows, axis=-1, keepdims=True)) + 1e-06)
    return (rows * scale * gain[None, :]).astype(jnp.bfloat16)

def reference(tokens, mix_gain, mlp_gain, query_weight, key_weight, value_weight, gate_weight, out_weight, up_weight, down_weight, query_scale, key_scale, value_scale, gate_scale, out_scale, up_scale, down_scale, forget):
    stream = tokens.astype(jnp.float32).T
    normed = norm_rows(stream, mix_gain)

    def project(weight, scale):
        product = jnp.dot(normed, weight.astype(jnp.bfloat16), preferred_element_type=jnp.float32)
        return (product * scale[None, :]).astype(jnp.bfloat16)
    shape = (N_FS, LEN, HEADS, HEAD_DIM)
    query = project(query_weight, query_scale).reshape(shape)
    key = project(key_weight, key_scale).reshape(shape)
    value = project(value_weight, value_scale).reshape(shape)
    gate = project(gate_weight, gate_scale).reshape(shape)
    mixed_heads = retain(query, key, value, gate, forget).reshape(TOKENS, RET_W).astype(jnp.bfloat16)
    out_b = out_weight.astype(jnp.bfloat16)
    group = RET_W // N_TP

    def mix_group(carry, index):
        rows = lax.dynamic_slice_in_dim(mixed_heads, index * group, group, 1)
        weight = lax.dynamic_slice_in_dim(out_b, index * group, group, 0)
        part = jnp.dot(rows, weight, preferred_element_type=jnp.float32).astype(jnp.bfloat16)
        part = lax.optimization_barrier(part)
        return (carry + part.astype(jnp.float32), None)
    groups = jnp.arange(N_TP, dtype=jnp.int32)
    mix_total, _ = lax.scan(mix_group, jnp.zeros((TOKENS, D), jnp.float32), groups)
    after_mix = (stream + mix_total * out_scale[None, :]).astype(jnp.bfloat16)
    normed_mlp = norm_rows(after_mix.astype(jnp.float32), mlp_gain)
    units = FF // N_TP

    def mlp_group(carry, index):
        w_up = lax.dynamic_slice_in_dim(up_weight, index * units, units, 1).astype(jnp.bfloat16)
        s_up = lax.dynamic_slice_in_dim(up_scale, index * units, units, 0)
        hidden = jnp.dot(normed_mlp, w_up, preferred_element_type=jnp.float32) * s_up[None, :]
        hidden = jnp.square(jax.nn.relu(hidden)).astype(jnp.bfloat16)
        w_down = lax.dynamic_slice_in_dim(down_weight, index * units, units, 0).astype(jnp.bfloat16)
        part = jnp.dot(hidden, w_down, preferred_element_type=jnp.float32).astype(jnp.bfloat16)
        part = lax.optimization_barrier(part)
        return (carry + part.astype(jnp.float32), None)
    mlp_total, _ = lax.scan(mlp_group, jnp.zeros((TOKENS, D), jnp.float32), groups)
    layer_out = (after_mix.astype(jnp.float32) + mlp_total * down_scale[None, :]).astype(jnp.bfloat16)
    return layer_out.T
```

```python
import functools

import jax
import jax.numpy as jnp
import numpy as np
from jax import lax
from jax.experimental import pallas as pl
from jax.experimental.pallas import tpu as pltpu
from jax.sharding import PartitionSpec as P

MESH = pl.DeviceIdType.MESH
BF = jnp.bfloat16
F32 = jnp.float32


def nn(a, b):
    return lax.dot_general(a, b, (((1,), (0,)), ((), ())), preferred_element_type=F32)


def nt(a, b):
    return lax.dot_general(a, b, (((1,), (1,)), ((), ())), preferred_element_type=F32)


def kernel(cfg, *refs):
    Z, X, Y, C, G, heads = cfg
    n_tp = Y * C
    n_w = 4
    tok, gains, scales, cos_t, sin_t, forget = refs[:6]
    own = refs[6 : 6 + n_w]
    out_ref = refs[6 + n_w]
    rest = refs[7 + n_w :]
    full = rest[:n_w]
    (scale_g, scale_row, tok_g, seqs, parts, core_in, y_out, y_in, z_out, z_in, normed, proj, mixed, hidden,
     local_sem, zs, zr, xs, xr, ts, tr, azs, azr, ays, ayr, acs, acr, rcs, rcr, rys, ryr, rzs, rzr) = rest[n_w:]
    me = lax.axis_index("fs")
    tp = lax.axis_index("tp")
    z = me // X
    x = lax.rem(me, X)
    y = tp // C
    core = lax.rem(tp, C)
    length, width = tok.shape
    ret = mixed.shape[1]
    head = ret // heads

    def at_z(o):
        return lax.rem(z + o, Z) * X + x

    def at_g(o):
        return (z // G * G + lax.rem(z + o, G)) * X + x

    def at_x(o):
        return z * X + lax.rem(x + o, X)

    def at_tp(o):
        return lax.rem(tp + o, n_tp)

    def at_y(o):
        return lax.rem(y + o, Y) * C + core

    def at_core(o):
        return y * C + lax.rem(core + o, C)

    barrier = pltpu.get_barrier_semaphore()
    for o in range(1, Z):
        pl.semaphore_signal(barrier, inc=1, device_id={"fs": at_z(o)}, device_id_type=MESH)
    for o in range(1, X):
        pl.semaphore_signal(barrier, inc=1, device_id={"fs": at_x(o)}, device_id_type=MESH)
    for o in range(1, n_tp):
        pl.semaphore_signal(barrier, inc=1, device_id={"tp": at_tp(o)}, device_id_type=MESH)
    pl.semaphore_wait(barrier, Z - 1 + X - 1 + n_tp - 1)

    pending = []

    def remote(src, dst, ss, rs, where):
        return pltpu.make_async_remote_copy(
            src_ref=src, dst_ref=dst, send_sem=ss, recv_sem=rs, device_id=where, device_id_type=MESH
        )

    def send(*parts_of):
        copy = remote(*parts_of)
        copy.start()
        pending.append(copy)

    def place(w, owner):
        if w == n_w:
            return scale_g.at[owner]
        rows = own[w].shape[-2]
        return full[w].at[pl.ds(pl.multiple_of(owner * rows, rows), rows)]

    def mine(w, o):
        if w == n_w:
            return scales
        return own[w].at[lax.rem(z + o, G)] if w >= 2 else own[w]

    def z_send(w):
        for o in range(1, Z):
            send(mine(w, o), place(w, me), zs.at[w, o - 1], zr.at[w, o - 1], {"fs": at_z(o)})

    def x_own(w):
        for o in range(1, X):
            send(mine(w, 0), place(w, me), xs.at[w, 0, o - 1], xr.at[w, 0, o - 1], {"fs": at_x(o)})

    def relay(w):
        for k in range(1, Z):
            piece = place(w, at_z(Z - k))
            remote(piece, piece, zs.at[w, k - 1], zr.at[w, k - 1], {"fs": at_z(k)}).wait_recv()
            for o in range(1, X):
                send(piece, piece, xs.at[w, k, o - 1], xr.at[w, k, o - 1], {"fs": at_x(o)})

    def finish(w):
        for k in range(Z):
            for o in range(1, X):
                owner = lax.rem(z + Z - k, Z) * X + lax.rem(x + X - o, X)
                piece = place(w, owner)
                remote(piece, piece, xs.at[w, k, o - 1], xr.at[w, k, o - 1], {"fs": at_x(o)}).wait_recv()

    def store_parts(k, t, value):
        parts[k, t % C, t // C] = value.astype(BF)

    def reduce_start(k):
        for o in range(1, C):
            send(parts.at[k, lax.rem(core + o, C)], core_in.at[k, o - 1], rcs.at[k, o - 1], rcr.at[k, o - 1],
                 {"tp": at_core(o)})

    def reduce_core(k):
        for o in range(1, C):
            slot = core_in.at[k, o - 1]
            remote(slot, slot, rcs.at[k, o - 1], rcr.at[k, o - 1], {"tp": at_core(o)}).wait_recv()
        for j in range(Y):
            value = parts[k, core, j].astype(F32)
            for o in range(1, C):
                value += core_in[k, o - 1, j].astype(F32)
            y_out[k, j] = value.astype(BF)
        for j in range(1, Y):
            send(y_out.at[k, lax.rem(y + j, Y)], y_in.at[k, j - 1], rys.at[k, j - 1], ryr.at[k, j - 1],
                 {"tp": at_y(j)})

    def reduce_y(k):
        value = y_out[k, y].astype(F32)
        for j in range(1, Y):
            slot = y_in.at[k, j - 1]
            remote(slot, slot, rys.at[k, j - 1], ryr.at[k, j - 1], {"tp": at_y(j)}).wait_recv()
            value += y_in[k, j - 1].astype(F32)
        return value

    def norm(block, row):
        square = jnp.zeros((length, 1), F32)
        for t in range(n_tp):
            v = block(t)[...].astype(F32)
            square += jnp.sum(v * v, axis=-1, keepdims=True)
        factor = lax.rsqrt(square / (width * n_tp) + 1e-6)
        for t in range(n_tp):
            cols = slice(t * width, (t + 1) * width)
            normed[:, cols] = (block(t)[...].astype(F32) * factor * gains[row : row + 1, cols]).astype(BF)

    for o in range(1, n_tp):
        send(tok, tok_g.at[tp], ts.at[o - 1], tr.at[o - 1], {"tp": at_tp(o)})
    for w in (n_w, 0, 1):
        z_send(w)
        x_own(w)
    locals_ = [pltpu.make_async_copy(mine(w, 0), place(w, me), local_sem.at[w]) for w in range(n_w + 1)]
    locals_.append(pltpu.make_async_copy(tok, tok_g.at[tp], local_sem.at[n_w + 1]))
    for copy in locals_:
        copy.start()
    for copy in locals_:
        copy.wait()
    for o in range(1, n_tp):
        slot = tok_g.at[at_tp(n_tp - o)]
        remote(slot, slot, ts.at[o - 1], tr.at[o - 1], {"tp": at_tp(o)}).wait_recv()
    norm(lambda t: tok_g.at[t], 0)

    relay(n_w)
    relay(0)
    relay(1)
    z_send(2)
    finish(n_w)
    finish(0)
    x_own(2)
    scale = jnp.sum(scale_g[...], axis=0)
    scale_row[...] = scale
    at = 4 * ret
    out_scale = scale[:, at : at + width]
    down_scale = scale[:, at + width : at + 2 * width]
    up_at = at + 2 * width

    for i in range(4):
        piece = nn(normed[...], full[0][:, i * ret : (i + 1) * ret])
        proj[i] = (piece * scale[:, i * ret : (i + 1) * ret]).astype(BF)

    r = lax.broadcasted_iota(jnp.int32, (ret, ret), 0)
    c = lax.broadcasted_iota(jnp.int32, (ret, ret), 1)
    odd = lax.rem(c, 2) == 1
    swap = jnp.where((r == c - 1) & odd, 1.0, jnp.where((r == c + 1) & ~odd, -1.0, 0.0)).astype(BF)
    same = jnp.where(r // head == c // head, 1.0 / head, 0.0).astype(F32)

    def turn(field):
        return field.astype(F32) * cos_t[...] + nn(field, swap) * sin_t[...]

    rot_q = turn(proj[0])
    rot_k = (turn(proj[1]) * head ** (-0.5)).astype(BF)
    vals = proj[2]
    rows = lax.broadcasted_iota(jnp.int32, (length, length), 0)
    cols = lax.broadcasted_iota(jnp.int32, (length, length), 1)
    dist = (rows - cols).astype(F32)
    lane = lax.broadcasted_iota(jnp.int32, (length, ret), 1) // head
    total = jnp.zeros((length, ret), F32)
    for h in range(heads):
        q_h = jnp.where(lane == h, rot_q, 0.0).astype(BF)
        decay = jnp.where(dist >= 0.0, jnp.exp(-forget[h] * jnp.maximum(dist, 0.0)), 0.0)
        inner = (nt(q_h, rot_k) * decay).astype(BF)
        total = jnp.where(lane == h, nn(inner, vals), total)
    mean = lax.dot_general(
        total * total, same, (((1,), (0,)), ((), ())), precision=lax.Precision.HIGHEST, preferred_element_type=F32
    )
    gate = proj[3].astype(F32)
    mixed[...] = (gate / (1.0 + jnp.exp(-gate)) * (total * lax.rsqrt(mean + 0.01))).astype(BF)

    finish(1)
    x_own(3)
    for t in range(n_tp):
        store_parts(G, t, nt(mixed[...], full[1][t * width : (t + 1) * width, :]))
    reduce_start(G)
    reduce_core(G)
    after = (tok[...].astype(F32) + reduce_y(G) * out_scale).astype(BF)
    seqs[0, tp] = after

    for k in range(1, G):
        send(seqs.at[0, tp], seqs.at[k, tp], azs.at[k - 1], azr.at[k - 1], {"fs": at_g(k)})

    def collect_z(k):
        slot = seqs.at[k, tp]
        if k:
            remote(slot, slot, azs.at[k - 1], azr.at[k - 1], {"fs": at_g(k)}).wait_recv()
        for j in range(1, Y):
            send(slot, slot, ays.at[k, j - 1], ayr.at[k, j - 1], {"tp": at_y(j)})
        for o in range(1, C):
            send(slot, slot, acs.at[k, 0, o - 1], acr.at[k, 0, o - 1], {"tp": at_core(o)})

    def collect_y(k):
        for j in range(1, Y):
            slot = seqs.at[k, at_y(Y - j)]
            remote(slot, slot, ays.at[k, j - 1], ayr.at[k, j - 1], {"tp": at_y(j)}).wait_recv()
            for o in range(1, C):
                send(slot, slot, acs.at[k, j, o - 1], acr.at[k, j, o - 1], {"tp": at_core(o)})

    def feed(k):
        for j in range(Y):
            for o in range(1, C):
                slot = seqs.at[k, lax.rem(y + Y - j, Y) * C + lax.rem(core + C - o, C)]
                remote(slot, slot, acs.at[k, j, o - 1], acr.at[k, j, o - 1], {"tp": at_core(o)}).wait_recv()
        norm(lambda t: seqs.at[k, t], 1)

    def expand(k):
        chunk = hidden.shape[2]
        step = 256 if chunk % 256 == 0 else chunk

        def tile(i, carry):
            here = pl.ds(pl.multiple_of(i * step, step), step)
            s = scale_row[:, pl.ds(pl.multiple_of(up_at + lax.rem(z, G) * chunk + i * step, 128), step)]
            u = jnp.maximum(nn(normed[...], full[2][:, here]) * s, 0.0)
            hidden[k, :, here] = (u * u).astype(BF)
            return carry

        lax.fori_loop(0, chunk // step, tile, 0)

    def shrink(k):
        for t in range(n_tp):
            store_parts(k, t, nt(hidden[k], full[3][t * width : (t + 1) * width, :]))
        reduce_start(k)

    def give_z(k):
        value = reduce_y(k)
        z_out[k] = value.astype(BF)
        if k:
            send(z_out.at[k], z_in.at[k - 1], rzs.at[k - 1], rzr.at[k - 1], {"fs": at_g(G - k)})

    collect_z(0)
    relay(2)
    for k in range(1, G):
        collect_z(k)
    z_send(3)
    collect_y(0)
    feed(0)
    finish(2)
    expand(0)
    for k in range(1, G):
        collect_y(k)
        feed(k)
        expand(k)
    relay(3)
    finish(3)
    order = list(range(1, G)) + [0]
    for k in order:
        shrink(k)
    for k in order:
        reduce_core(k)
    for k in order:
        give_z(k)
    mlp_total = z_out[0].astype(F32)
    for k in range(1, G):
        slot = z_in.at[k - 1]
        remote(slot, slot, rzs.at[k - 1], rzr.at[k - 1], {"fs": at_g(k)}).wait_recv()
        mlp_total += z_in[k - 1].astype(F32)
    out_ref[...] = (seqs[0, tp].astype(F32) + mlp_total * down_scale).astype(BF)
    for copy in pending:
        copy.wait_send()


def tables(length, head, heads):
    half = head // 2
    inverse = 1.0 / 10000.0 ** np.linspace(0.0, 1.0, half)
    angle = np.arange(length)[:, None] * inverse.astype(np.float32).astype(np.float64)[None, :]
    spread = lambda a: np.tile(np.repeat(a, 2, axis=1), (1, heads)).astype(np.float32)
    return spread(np.cos(angle)), spread(np.sin(angle))


def solution(mesh):
    n_fs, n_tp = mesh.shape["fs"], mesh.shape["tp"]
    heights = [getattr(d, "coords", (0, 0, i))[2] for i, d in enumerate(mesh.devices[:, 0])]
    X = heights.count(heights[0])
    if n_fs % X:
        X = 1
    Z = n_fs // X
    cores = [getattr(d, "core_on_chip", 0) for d in mesh.devices[0]]
    C = len(set(cores))
    if n_tp % C:
        C = 1
    Y = n_tp // C
    G = next(g for g in (4, 2, Z) if Z % g == 0)

    def on_device(tokens, mix_gain, mlp_gain, wq, wk, wv, wg, wo, wu, wd, sq, sk, sv, sg, so, su, sd, forget):
        width, length = tokens.shape
        D = width * n_tp
        ret = wq.shape[1]
        heads = forget.shape[0]
        ff = wu.shape[1]
        chunk = ff // G
        me = lax.axis_index("fs")

        def spot(s):
            wide = jnp.tile(s, n_fs)
            return jnp.where(jnp.arange(wide.shape[0]) // s.shape[0] == me, wide, 0.0)

        scales = jnp.concatenate([spot(s) for s in (sq, sk, sv, sg, so, sd, su)])[None, :]
        gains = jnp.stack([mix_gain, mlp_gain])
        cos_t, sin_t = tables(length, ret // heads, heads)
        own = [jnp.concatenate([w.astype(BF) for w in (wq, wk, wv, wg)], axis=1), wo.astype(BF).T]
        own.append(wu.astype(BF).reshape(-1, G, chunk).transpose(1, 0, 2))
        own.append(wd.astype(BF).reshape(G, chunk, -1).transpose(0, 2, 1))
        n_w = len(own)
        vm = pl.BlockSpec(memory_space=pltpu.VMEM)
        dma = pltpu.SemaphoreType.DMA
        tile = (length, width)
        scratch = [pltpu.VMEM((n_fs * w.shape[-2], w.shape[-1]), BF) for w in own]
        scratch += [
            pltpu.VMEM((n_fs,) + scales.shape, F32),
            pltpu.VMEM(scales.shape, F32),
            pltpu.VMEM((n_tp,) + tile, BF),
            pltpu.VMEM((G, n_tp) + tile, BF),
            pltpu.VMEM((G + 1, C, Y) + tile, BF),
            pltpu.VMEM((G + 1, C - 1, Y) + tile, BF),
            pltpu.VMEM((G + 1, Y) + tile, BF),
            pltpu.VMEM((G + 1, Y - 1) + tile, BF),
            pltpu.VMEM((G,) + tile, BF),
            pltpu.VMEM((G - 1,) + tile, BF),
            pltpu.VMEM((length, D), BF),
            pltpu.VMEM((4, length, ret), BF),
            pltpu.VMEM((length, ret), BF),
            pltpu.VMEM((G, length, chunk), BF),
            dma((n_w + 2,)),
        ]
        for shape in [(n_w + 1, Z - 1), (n_w + 1, Z, X - 1), (n_tp - 1,), (G - 1,), (G, Y - 1), (G, Y, C - 1),
                      (G + 1, C - 1), (G + 1, Y - 1), (G - 1,)]:
            scratch += [dma(shape), dma(shape)]
        out = pl.pallas_call(
            functools.partial(kernel, (Z, X, Y, C, G, heads)),
            out_shape=jax.ShapeDtypeStruct((length, width), BF),
            in_specs=[vm] * 5 + [pl.BlockSpec(memory_space=pltpu.SMEM)] + [vm] * n_w,
            out_specs=vm,
            scratch_shapes=scratch,
            compiler_params=pltpu.CompilerParams(
                collective_id=0, has_side_effects=True, vmem_limit_bytes=60 * 2**20
            ),
            name="layer",
        )(tokens.T, gains, scales, jnp.asarray(cos_t), jnp.asarray(sin_t), forget, *own)
        return out.T

    cut = P(("tp", "fs"))
    rows, cols = P("fs", "tp"), P("tp", "fs")
    in_specs = (cols, P(), P(), rows, rows, rows, rows, cols, rows, cols) + (cut,) * 7 + (P("tp"),)
    return jax.shard_map(on_device, mesh=mesh, in_specs=in_specs, out_specs=cols, check_vma=False)
```

```python
import functools

import jax
import jax.numpy as jnp
import numpy as np
from jax import lax
from jax.experimental import pallas as pl
from jax.experimental.pallas import tpu as pltpu
from jax.sharding import PartitionSpec as P

MESH = pl.DeviceIdType.MESH
BF = jnp.bfloat16
F32 = jnp.float32
LANES = 128


def nn(a, b):
    return lax.dot_general(a, b, (((1,), (0,)), ((), ())), preferred_element_type=F32)


def pick(table, at):
    value = jnp.int32(table[0])
    for a in range(1, len(table)):
        value = jnp.where(at == a, jnp.int32(table[a]), value)
    return value


def part_of(n):
    return min(n, LANES)


def scale_rows(s):
    n = s.shape[0]
    if n < LANES:
        return jnp.pad(s, (0, LANES - n))[None, :]
    return s.reshape(-1, LANES)


class Cfg:
    pass


def kernel(cfg, *refs):
    Z, X, Y, C, G = cfg.Z, cfg.X, cfg.Y, cfg.C, cfg.G
    n_tp, n_fs = Y * C, Z * X
    n_dev = n_tp * n_fs
    L, width, D, ret, hw, chunk, rows = cfg.L, cfg.width, cfg.D, cfg.ret, cfg.hw, cfg.chunk, cfg.rows
    head = cfg.head
    (tokens, gains, scales, cos_t, sin_t, forget, wq, wk, wv, wg, wo, wu, wd, out_ref) = refs[:14]
    (tok_g, mix_g, out_full, f_proj, f_up, f_down, o_proj, o_up, o_down, o_out, st_proj, st_out, st_up, st_down,
     parts, core_in, y_out, y_in, z_out, z_in, after, normed, hidden, keep, gain_c, out_c, up_c, down_c, proj_c,
     decay, scale_g, load_sem, local_sem, sc_s, sc_r, wzs, wzr, wxs, wxr,
     t_zs, t_zr, t_ys, t_yr, t_cs, t_cr, m_zs, m_zr, m_ys, m_yr, m_cs, m_cr,
     p_zs, p_zr, p_ys, p_yr, p_xs, p_xr, p_cs, p_cr, rcs, rcr, rys, ryr, rzs, rzr) = refs[14:]
    me = lax.axis_index("fs")
    tp = lax.axis_index("tp")
    z = me // X
    x = lax.rem(me, X)
    y = tp // C
    core = lax.rem(tp, C)
    flat = tp * n_fs + me
    g = lax.rem(z, G)
    base = z - g
    full = [f_proj, f_up, f_down]
    own = [o_proj, o_up, o_down]

    def to_z(zz):
        return {"fs": zz * X + x}

    def to_x(o):
        return {"fs": z * X + lax.rem(x + o, X)}

    def to_y(o):
        return {"tp": lax.rem(y + o, Y) * C + core}

    def to_core(o):
        return {"tp": y * C + lax.rem(core + o, C)}

    def peer(o):
        q = lax.rem(flat + o, n_dev)
        return {"fs": lax.rem(q, n_fs), "tp": q // n_fs}

    barrier = pltpu.get_barrier_semaphore()

    def greet(o, carry):
        pl.semaphore_signal(barrier, inc=1, device_id=peer(o), device_id_type=MESH)
        return carry

    lax.fori_loop(1, n_dev, greet, 0)

    def rows_of(i, n):
        return pl.ds(pl.multiple_of(i * n, n), n)

    own_tok = tok_g.at[g, rows_of(tp, width)]
    loads = [(tokens, own_tok)]
    loads += [(w, st_proj.at[i]) for i, w in enumerate((wq, wk, wv, wg))]
    loads += [(wo, st_out), (wu, st_up), (wd, st_down)]
    loads = [pltpu.make_async_copy(a, b, load_sem.at[i]) for i, (a, b) in enumerate(loads)]
    for copy in loads:
        copy.start()

    pending = []

    def remote(src, dst, ss, rs, where):
        return pltpu.make_async_remote_copy(
            src_ref=src, dst_ref=dst, send_sem=ss, recv_sem=rs, device_id=where, device_id_type=MESH
        )

    def send(*a, when=None):
        copy = remote(*a)
        if when is None:
            copy.start()
        else:
            pl.when(when)(copy.start)
        pending.append((copy, when))

    def arrived(ref, ss, rs):
        remote(ref, ref, ss, rs, to_core(1) if C > 1 else to_z(z)).wait_recv()

    class Spread:
        def __init__(self, n, at, first, ref, zs, zr, ys, yr, cs, cr, xs=None, xr=None):
            self.n, self.at, self.first, self.ref = n, at, first, ref
            self.zs, self.zr, self.ys, self.yr, self.cs, self.cr, self.xs, self.xr = zs, zr, ys, yr, cs, cr, xs, xr
            self.nx = X if xs is not None else 1

        def order(self, i):
            n = self.n
            return pick([sorted(range(n), key=lambda q: (abs(q - a), q))[i] for a in range(n)], self.at)

        def block(self, i, j, k, o):
            tps = lax.rem(y + Y - j, Y) * C + lax.rem(core + C - o, C)
            return self.ref(self.order(i), lax.rem(x + X - k, X), tps)

        def fan_y(self, i):
            piece = self.block(i, 0, 0, 0)
            for j in range(1, Y):
                send(piece, piece, self.ys.at[i, j - 1], self.yr.at[i, j - 1], to_y(j))

        def fan_x(self, i, j):
            piece = self.block(i, j, 0, 0)
            for k in range(1, self.nx):
                send(piece, piece, self.xs.at[i, j, k - 1], self.xr.at[i, j, k - 1], to_x(k))

        def fan_c(self, i, j, k):
            piece = self.block(i, j, k, 0)
            for o in range(1, C):
                send(piece, piece, self.cs.at[i, j, k, o - 1], self.cr.at[i, j, k, o - 1], to_core(o))

        def fan(self, i):
            self.fan_y(i)
            self.fan_x(i, 0)
            self.fan_c(i, 0, 0)

        def start(self):
            piece = self.block(0, 0, 0, 0)
            slot = self.zr.at[self.at]
            send(piece, piece, self.zs.at[0], slot, to_z(self.first + self.at + 1), when=self.at < self.n - 1)
            send(piece, piece, self.zs.at[self.n], slot, to_z(self.first + self.at - 1), when=self.at > 0)
            self.fan(0)

        def on_z(self, i):
            o = self.order(i)
            piece = self.block(i, 0, 0, 0)
            arrived(piece, self.zs.at[i], self.zr.at[o])
            nxt = jnp.where(o < self.at, self.at + 1, self.at - 1)
            send(piece, piece, self.zs.at[i], self.zr.at[o], to_z(self.first + nxt),
                 when=(nxt >= 0) & (nxt < self.n))
            self.fan(i)

        def on_y(self, i):
            for j in range(1, Y):
                arrived(self.block(i, j, 0, 0), self.ys.at[i, j - 1], self.yr.at[i, j - 1])
                self.fan_x(i, j)
                self.fan_c(i, j, 0)

        def on_x(self, i):
            for j in range(Y):
                for k in range(1, self.nx):
                    arrived(self.block(i, j, k, 0), self.xs.at[i, j, k - 1], self.xr.at[i, j, k - 1])
                    self.fan_c(i, j, k)

        def on_c(self, i):
            for j in range(Y):
                for k in range(self.nx):
                    for o in range(1, C):
                        arrived(self.block(i, j, k, o), self.cs.at[i, j, k, o - 1], self.cr.at[i, j, k, o - 1])

    tok = Spread(G, g, base, lambda zi, xi, t: tok_g.at[zi, rows_of(t, width)], t_zs, t_zr, t_ys, t_yr, t_cs, t_cr)
    mix = Spread(G, g, base, lambda zi, xi, t: mix_g.at[:, pl.ds(pl.multiple_of(t * ret + zi * hw, hw), hw)],
                 m_zs, m_zr, m_ys, m_yr, m_cs, m_cr)
    prj = Spread(Z, z, 0, lambda zi, xi, t: out_full.at[rows_of(zi * X + xi, rows), rows_of(t, ret)],
                 p_zs, p_zr, p_ys, p_yr, p_cs, p_cr, p_xs, p_xr)

    def place(w, owner):
        if w == 2:
            return full[w].at[rows_of(owner, rows)]
        if rows % LANES:
            return full[w].at[owner]
        return full[w].at[:, rows_of(owner, rows)]

    def mul(w, here, v):
        if rows % LANES:
            total = nn(full[w][0, here, :], v[0:rows, :])
            for f in range(1, n_fs):
                total += nn(full[w][f, here, :], v[f * rows : (f + 1) * rows, :])
            return total
        return nn(full[w][here, :], v[...])

    def z_send(w):
        for o in range(1, Z):
            to = lax.rem(z + o, Z)
            send(own[w].at[lax.rem(to, G)], place(w, me), wzs.at[w, o - 1], wzr.at[w, o - 1], to_z(to))

    def x_own(w):
        for o in range(1, X):
            send(own[w].at[g], place(w, me), wxs.at[w, 0, o - 1], wxr.at[w, 0, o - 1], to_x(o))
        copy = pltpu.make_async_copy(own[w].at[g], place(w, me), local_sem.at[w])
        copy.start()
        return copy

    def relay(w):
        for k in range(1, Z):
            piece = place(w, lax.rem(z + Z - k, Z) * X + x)
            arrived(piece, wzs.at[w, k - 1], wzr.at[w, k - 1])
            for o in range(1, X):
                send(piece, piece, wxs.at[w, k, o - 1], wxr.at[w, k, o - 1], to_x(o))

    def finish(w, local):
        local.wait()
        for k in range(Z):
            for o in range(1, X):
                owner = lax.rem(z + Z - k, Z) * X + lax.rem(x + X - o, X)
                arrived(place(w, owner), wxs.at[w, k, o - 1], wxr.at[w, k, o - 1])

    def wide(col, n):
        return jnp.concatenate([col] * (n // LANES), axis=1) if n > LANES else col[:, :n]

    def column(row):
        return jnp.broadcast_to(row, (LANES, LANES)).T

    def columns(dst, row, n, count, first):
        w = part_of(n)
        per = n // w

        def one(f, carry):
            for r in range(per):
                c = column(scale_g[first + f, row + r : row + r + 1, :])[:w]
                if w % 8 == 0:
                    dst[pl.ds(pl.multiple_of((f * per + r) * w, 8), w), :] = c
                else:
                    dst[f * w : (f + 1) * w, :] = c
            return carry

        if w % 8 == 0:
            lax.fori_loop(0, count, one, 0)
        else:
            for f in range(count):
                one(f, 0)

    loads[0].wait()
    scale_g[flat] = scales[...]
    pl.semaphore_wait(barrier, n_dev - 1)

    with jax.named_scope("start"):
        tok.start()

        def tell(o, carry):
            remote(scales, scale_g.at[flat], sc_s.at[o], sc_r.at[o], peer(o)).start()
            return carry

        lax.fori_loop(1, n_dev, tell, 0)

    with jax.named_scope("cast"):
        for i in range(4):
            loads[1 + i].wait()
            t = st_proj[i].T
            for k in range(G):
                o_proj[k, i * hw : (i + 1) * hw, :] = t[k * hw : (k + 1) * hw, :].astype(BF)
        z_send(0)
        local0 = x_own(0)
        loads[5].wait()
        own_out = out_full.at[rows_of(me, rows), rows_of(tp, ret)]
        o_out[...] = st_out[...].T.astype(BF)
        copy = pltpu.make_async_copy(o_out, own_out, local_sem.at[3])
        copy.start()
        copy.wait()
        loads[6].wait()
        loads[7].wait()
        step = min(chunk, 512)

        def cast_up(k, carry):
            here = rows_of(k, step)
            o_up[k * step // chunk, pl.ds(pl.multiple_of(lax.rem(k * step, chunk), step), step), :] = (
                st_up[:, here].T.astype(BF))
            o_down[k * step // chunk, :, pl.ds(pl.multiple_of(lax.rem(k * step, chunk), step), step)] = (
                st_down[here, :].T.astype(BF))
            return carry

        lax.fori_loop(0, G * chunk // step, cast_up, 0)

    with jax.named_scope("tables"):
        def gain_row(i, carry):
            gain_c[rows_of(i, LANES), :] = column(gains[pl.ds(i, 1), :])
            return carry

        lax.fori_loop(0, 2 * D // LANES, gain_row, 0)
        krow = lax.broadcasted_iota(jnp.int32, (L, L), 0)
        qcol = lax.broadcasted_iota(jnp.int32, (L, L), 1)
        dist = (qcol - krow).astype(F32)
        for h in range(hw // head):
            rate = forget[g * (hw // head) + h]
            decay[h] = jnp.where(dist >= 0.0, jnp.exp(-rate * jnp.maximum(dist, 0.0)), 0.0)

    with jax.named_scope("tok1"):
        tok.on_z(1)
        tok.on_y(0)
    with jax.named_scope("prj0"):
        prj.start()
    with jax.named_scope("relay0"):
        relay(0)
    for i in range(2, G):
        with jax.named_scope("tok%d" % i):
            tok.on_z(i)
            tok.on_y(i - 1)
    with jax.named_scope("scales"):
        def heard(o, carry):
            slot = scale_g.at[lax.rem(flat + n_dev - o, n_dev)]
            arrived(slot, sc_s.at[o], sc_r.at[o])
            return carry

        lax.fori_loop(1, n_dev, heard, 0)
        for i in range(4):
            columns(proj_c.at[i], i, ret // n_fs, n_fs, tp * n_fs)
        columns(out_c, 4, D // n_dev, n_dev, 0)
        columns(down_c, 5, width // n_fs, n_fs, tp * n_fs)
        columns(up_c, 6, G * chunk // n_fs, n_fs, tp * n_fs)

    with jax.named_scope("finish0"):
        finish(0, local0)
    z_send(1)
    local1 = x_own(1)

    tile = 256 if D % 256 == 0 else D
    r64 = lax.broadcasted_iota(jnp.int32, (head, head), 0)
    c64 = lax.broadcasted_iota(jnp.int32, (head, head), 1)
    odd = lax.rem(r64, 2) == 1
    swap = jnp.where((c64 == r64 - 1) & odd, 1.0, jnp.where((c64 == r64 + 1) & ~odd, -1.0, 0.0)).astype(BF)

    def scaled(src, square, gain_at):
        factor = lax.rsqrt(square / D + 1e-6)

        def one(t, carry):
            here = rows_of(t, tile)
            gain = wide(gain_c[pl.ds(pl.multiple_of(gain_at + t * tile, tile), tile), :], L)
            normed[here, :] = (src[here, :].astype(F32) * factor * gain).astype(BF)
            return carry

        lax.fori_loop(0, D // tile, one, 0)

    def turn(field):
        return field.astype(F32) * cos_t[...] + nn(swap, field) * sin_t[...]

    def attend(i):
        s = tok.order(i)
        src = tok_g.at[s]

        def add(t, square):
            v = src[rows_of(t, tile), :].astype(F32)
            return square + jnp.sum(v * v, axis=0, keepdims=True)

        scaled(src, lax.fori_loop(0, D // tile, add, jnp.zeros((1, L), F32)), 0)
        proj = mul(0, slice(0, 4 * hw), normed)
        heads_at = pl.ds(pl.multiple_of(g * hw, hw), hw)
        q, k, v, gate = [
            (proj[n * hw : (n + 1) * hw, :] * wide(proj_c[n, heads_at, :], L)).astype(BF) for n in range(4)
        ]
        for h in range(hw // head):
            at = slice(h * head, (h + 1) * head)
            rot_q = turn(q[at]).astype(BF)
            rot_k = (turn(k[at]) * head ** (-0.5)).T.astype(BF)
            inner = (nn(rot_k, rot_q) * decay[h]).astype(BF)
            total = nn(v[at], inner)
            mean = jnp.sum(total * total, axis=0, keepdims=True) / head
            f = gate[at].astype(F32)
            value = f / (1.0 + jnp.exp(-f)) * (total * lax.rsqrt(mean + 0.01))
            mix_g[s, pl.ds(pl.multiple_of(tp * ret + g * hw + h * head, head), head), :] = value.astype(BF)

    for i in range(G):
        with jax.named_scope("att%d" % i):
            if i == G - 1:
                tok.on_y(i)
            tok.on_c(i)
            attend(i)
            if i == 0:
                for k in range(1, Z):
                    prj.on_z(k)
    with jax.named_scope("mix_start"):
        mix.start()
    with jax.named_scope("prj_y"):
        for k in range(Z):
            prj.on_y(k)
    with jax.named_scope("relay1"):
        relay(1)
    with jax.named_scope("mix_z"):
        for i in range(1, G):
            mix.on_z(i)
    z_send(2)
    local2 = x_own(2)
    with jax.named_scope("prj_x"):
        for k in range(Z):
            prj.on_x(k)
    with jax.named_scope("mix_y"):
        for i in range(G):
            mix.on_y(i)
    with jax.named_scope("prj_c"):
        for k in range(Z):
            prj.on_c(k)
    with jax.named_scope("finish1"):
        finish(1, local1)
    with jax.named_scope("mix_c"):
        for i in range(G):
            mix.on_c(i)

    def expand(i):
        s = tok.order(i)

        def mixed(t, square):
            here = rows_of(t, tile)
            v = nn(out_full[here, :], mix_g[s]) * wide(out_c[here, :], L)
            a = (tok_g[s, here, :].astype(F32) + v).astype(BF)
            after[here, :] = a
            a = a.astype(F32)
            return square + jnp.sum(a * a, axis=0, keepdims=True)

        scaled(after, lax.fori_loop(0, D // tile, mixed, jnp.zeros((1, L), F32)), D)
        if i == 0:
            keep[...] = after[rows_of(tp, width), :]
        ut = 256 if chunk % 256 == 0 else chunk

        def units(t, carry):
            here = rows_of(t, ut)
            sc = wide(up_c[pl.ds(pl.multiple_of(g * chunk + t * ut, ut), ut), :], L)
            u = jnp.maximum(mul(1, here, normed) * sc, 0.0)
            hidden[i, here, :] = (u * u).astype(BF)
            return carry

        lax.fori_loop(0, chunk // ut, units, 0)

    def block_rows(j, c):
        return rows_of(j * C + c, width)

    def shrink(i):
        def one(t, carry):
            here = rows_of(t, tile)
            parts[i, here, :] = nn(full[2][here, :], hidden[i]).astype(BF)
            return carry

        lax.fori_loop(0, D // tile, one, 0)
        for o in range(1, C):
            for j in range(Y):
                send(parts.at[i, block_rows(j, lax.rem(core + o, C))], core_in.at[i, o - 1, j],
                     rcs.at[i, o - 1, j], rcr.at[i, o - 1, j], to_core(o))

    def reduce_core(i):
        for o in range(1, C):
            for j in range(Y):
                arrived(core_in.at[i, o - 1, j], rcs.at[i, o - 1, j], rcr.at[i, o - 1, j])
        for j in range(Y):
            value = parts[i, block_rows(j, core), :].astype(F32)
            for o in range(1, C):
                value += core_in[i, o - 1, j].astype(F32)
            y_out[i, j] = value.astype(BF)
        for j in range(1, Y):
            send(y_out.at[i, lax.rem(y + j, Y)], y_in.at[i, j - 1], rys.at[i, j - 1], ryr.at[i, j - 1], to_y(j))

    def reduce_y(i):
        value = y_out[i, y].astype(F32)
        for j in range(1, Y):
            arrived(y_in.at[i, j - 1], rys.at[i, j - 1], ryr.at[i, j - 1])
            value += y_in[i, j - 1].astype(F32)
        if i:
            z_out[i] = value.astype(BF)
            send(z_out.at[i], z_in.at[g], rzs.at[i], rzr.at[g], to_z(base + tok.order(i)))
        return value

    order = list(range(G - 1, -1, -1))
    for i in order[::-1]:
        with jax.named_scope("expand%d" % i):
            expand(i)
            if i == 0:
                relay(2)
    with jax.named_scope("finish2"):
        finish(2, local2)
    for n, i in enumerate(order):
        with jax.named_scope("shrink%d" % i):
            shrink(i)
            if n:
                reduce_core(order[n - 1])
    with jax.named_scope("reduce"):
        reduce_core(order[-1])
        for i in order:
            total = reduce_y(i)
    with jax.named_scope("final"):
        for i in range(1, G):
            o = tok.order(i)
            arrived(z_in.at[o], rzs.at[i], rzr.at[o])
            total += z_in[o].astype(F32)
        out_ref[...] = (keep[...].astype(F32) + total * wide(down_c[...], L)).astype(BF)
    for copy, when in pending:
        if when is None:
            copy.wait_send()
        else:
            pl.when(when)(copy.wait_send)

    def told(o, carry):
        remote(scales, scale_g.at[flat], sc_s.at[o], sc_r.at[o], peer(o)).wait_send()
        return carry

    lax.fori_loop(1, n_dev, told, 0)


def tables(length, head):
    half = head // 2
    inverse = 1.0 / 10000.0 ** np.linspace(0.0, 1.0, half)
    angle = np.arange(length)[:, None] * inverse.astype(np.float32).astype(np.float64)[None, :]
    spread = lambda a: np.repeat(a, 2, axis=1).T.astype(np.float32)
    return spread(np.cos(angle)), spread(np.sin(angle))


def solution(mesh):
    n_fs, n_tp = mesh.shape["fs"], mesh.shape["tp"]
    heights = [getattr(d, "coords", (0, 0, i))[2] for i, d in enumerate(mesh.devices[:, 0])]
    X = heights.count(heights[0])
    if n_fs % X:
        X = 1
    Z = n_fs // X
    cores = [getattr(d, "core_on_chip", 0) for d in mesh.devices[0]]
    C = len(set(cores))
    if n_tp % C:
        C = 1
    Y = n_tp // C

    def on_device(tokens, mix_gain, mlp_gain, wq, wk, wv, wg, wo, wu, wd, sq, sk, sv, sg, so, su, sd, forget):
        cfg = Cfg()
        cfg.Z, cfg.X, cfg.Y, cfg.C = Z, X, Y, C
        width, L = tokens.shape
        cfg.width, cfg.L, cfg.D = width, L, width * n_tp
        D = cfg.D
        heads = forget.shape[0]
        G = cfg.G = next(q for q in (4, 2, 1) if Z % q == 0 and heads % q == 0)
        ret = cfg.ret = wq.shape[1]
        cfg.head = ret // heads
        hw = cfg.hw = ret // G
        chunk = cfg.chunk = wu.shape[1] // G
        rows = cfg.rows = wq.shape[0]
        n_dev = n_fs * n_tp
        scales = jnp.concatenate([scale_rows(s) for s in (sq, sk, sv, sg, so, sd, su)])
        scales = jnp.pad(scales, ((0, -scales.shape[0] % 8), (0, 0)))
        gains = jnp.concatenate([mix_gain, mlp_gain]).reshape(-1, LANES)
        cos_t, sin_t = tables(L, cfg.head)
        vm = pl.BlockSpec(memory_space=pltpu.VMEM)
        hbm = pl.BlockSpec(memory_space=pl.ANY)
        dma = pltpu.SemaphoreType.DMA
        strided = rows % LANES == 0
        vmem = lambda *shape, t=BF: pltpu.VMEM(shape, t)
        stack = (lambda n: vmem(n, D)) if strided else (lambda n: vmem(n_fs, n, rows))
        scratch = [
            vmem(G, D, L), vmem(G, ret * n_tp, L), vmem(D, ret * n_tp), stack(4 * hw), stack(chunk), vmem(D, chunk),
            vmem(G, 4 * hw, rows), vmem(G, chunk, rows), vmem(G, rows, chunk), vmem(rows, ret),
            vmem(4, rows, ret, t=F32), vmem(*wo.shape, t=F32), vmem(*wu.shape, t=F32), vmem(*wd.shape, t=F32),
            vmem(G, D, L), vmem(G, max(C - 1, 1), Y, width, L), vmem(G, Y, width, L),
            vmem(G, max(Y - 1, 1), width, L), vmem(G, width, L), vmem(G, width, L),
            vmem(D, L), vmem(D, L), vmem(G, chunk, L), vmem(width, L),
            vmem(2 * D, LANES, t=F32), vmem(D, LANES, t=F32), vmem(G * chunk, LANES, t=F32),
            vmem(width, LANES, t=F32), vmem(4, ret, LANES, t=F32), vmem(hw // cfg.head, L, L, t=F32),
            vmem(n_dev, *scales.shape, t=F32), dma((8,)), dma((4,)),
        ]
        line = lambda n, nx: [(n + 1,), (n,), (n, Y), (n, Y), (n, Y, nx, C), (n, Y, nx, C)]
        shapes = [(n_dev,), (n_dev,), (3, Z), (3, Z), (3, Z, X), (3, Z, X)] + line(G, 1) + line(G, 1)
        first = line(Z, X)
        shapes += first[:4] + [(Z, Y, X), (Z, Y, X)] + first[4:]
        shapes += [(G, C, Y), (G, C, Y), (G, Y), (G, Y), (G,), (G,)]
        scratch += [dma(s) for s in shapes]
        return pl.pallas_call(
            functools.partial(kernel, cfg),
            out_shape=jax.ShapeDtypeStruct((width, L), BF),
            in_specs=[hbm] + [vm] * 4 + [pl.BlockSpec(memory_space=pltpu.SMEM)] + [hbm] * 7,
            out_specs=vm,
            scratch_shapes=scratch,
            compiler_params=pltpu.CompilerParams(
                collective_id=0, has_side_effects=True, vmem_limit_bytes=60 * 2**20
            ),
            name="layer",
        )(tokens, gains, scales, jnp.asarray(cos_t), jnp.asarray(sin_t), forget, wq, wk, wv, wg, wo, wu, wd)

    cut = P(("tp", "fs"))
    rows, cols = P("fs", "tp"), P("tp", "fs")
    in_specs = (cols, P(), P(), rows, rows, rows, rows, cols, rows, cols) + (cut,) * 7 + (P("tp"),)
    return jax.shard_map(on_device, mesh=mesh, in_specs=in_specs, out_specs=cols, check_vma=False)
```

```python
import functools
import math

import jax
import jax.numpy as jnp
import numpy as np
from jax import lax
from jax.experimental import pallas as pl
from jax.experimental.pallas import tpu as pltpu
from jax.sharding import PartitionSpec as P

MESH = pl.DeviceIdType.MESH
BF = jnp.bfloat16
F32 = jnp.float32
LANES = 128


def nn(a, b):
    return lax.dot_general(a, b, (((1,), (0,)), ((), ())), preferred_element_type=F32)


def pick(table, at):
    value = jnp.int32(table[0])
    for a in range(1, len(table)):
        value = jnp.where(at == a, jnp.int32(table[a]), value)
    return value


def part_of(n):
    return min(n, LANES)


def scale_rows(s):
    n = s.shape[0]
    return s.reshape(-1, part_of(n))


class Cfg:
    pass


def kernel(cfg, *refs):
    Z, X, Y, C, G = cfg.Z, cfg.X, cfg.Y, cfg.C, cfg.G
    n_tp, n_fs = Y * C, Z * X
    n_dev = n_tp * n_fs
    L, width, D, ret, hw, chunk, rows = cfg.L, cfg.width, cfg.D, cfg.ret, cfg.hw, cfg.chunk, cfg.rows
    head, Q, U = cfg.head, cfg.Q, cfg.U
    rq, uh = rows // Q, chunk // U
    DOWN = 1 + U
    (tokens, mix_gain, mlp_gain, cos_t, sin_t, forget, wq, wk, wv, wg, wo, wu, wd) = refs[:13]
    own_scales, out_ref = refs[13:20], refs[20]
    (tok_g, mix_g, out_full, f_proj, f_up, f_down, o_proj, o_up, o_down, o_out, st_proj, st_out, st_up, st_down,
     parts, core_in, y_out, y_in, z_out, z_in, after, normed, hidden, keep, gain_c, out_c, up_c, down_c, proj_c,
     decay, scale_g, load_sem, local_sem, sc_s, sc_r, wzs, wzr, wxs, wxr,
     t_zs, t_zr, t_ys, t_yr, t_cs, t_cr, m_zs, m_zr, m_ys, m_yr, m_cs, m_cr,
     p_zs, p_zr, p_ys, p_yr, p_xs, p_xr, p_cs, p_cr, rcs, rcr, rys, ryr, rzs, rzr, ncs, ncr, scales) = refs[21:]
    me = lax.axis_index("fs")
    tp = lax.axis_index("tp")
    z = me // X
    x = lax.rem(me, X)
    y = tp // C
    core = lax.rem(tp, C)
    flat = tp * n_fs + me
    g = lax.rem(z, G)
    base = z - g
    strided = rows % LANES == 0

    def to_z(zz):
        return {"fs": zz * X + x}

    def to_x(o):
        return {"fs": z * X + lax.rem(x + o, X)}

    def to_y(o):
        return {"tp": lax.rem(y + o, Y) * C + core}

    def to_core(o):
        return {"tp": y * C + lax.rem(core + o, C)}

    def peer(o):
        q = lax.rem(flat + o, n_dev)
        return {"fs": lax.rem(q, n_fs), "tp": q // n_fs}

    barrier = pltpu.get_barrier_semaphore()

    def greet(o, carry):
        pl.semaphore_signal(barrier, inc=1, device_id=peer(o), device_id_type=MESH)
        return carry

    lax.fori_loop(1, n_dev, greet, 0)

    def rows_of(i, n):
        return pl.ds(pl.multiple_of(i * n, n), n)

    def seq_at(s):
        return pl.ds(pl.multiple_of(s * L, LANES), L)

    own_tok = tok_g.at[rows_of(tp, width), seq_at(g)]
    loads = [(tokens, own_tok)]
    loads += [(w, st_proj.at[i]) for i, w in enumerate((wq, wk, wv, wg))]
    loads += [(wo, st_out), (wu, st_up), (wd, st_down)]
    loads = [pltpu.make_async_copy(a, b, load_sem.at[i]) for i, (a, b) in enumerate(loads)]
    for copy in loads:
        copy.start()

    pending = []

    def remote(src, dst, ss, rs, where):
        return pltpu.make_async_remote_copy(
            src_ref=src, dst_ref=dst, send_sem=ss, recv_sem=rs, device_id=where, device_id_type=MESH
        )

    def emit(waits, copies, when=None, track=True):
        def go():
            for copy in waits:
                copy.wait_recv()
            for copy, ok in copies:
                if ok is None:
                    copy.start()
                else:
                    pl.when(ok)(copy.start)

        if when is None:
            go()
        else:
            pl.when(when)(go)
        if track:
            pending.extend(copies)

    def send(*a):
        emit([], [(remote(*a), None)])

    def arrived(ref, ss, rs):
        remote(ref, ref, ss, rs, to_core(1) if C > 1 else to_z(z)).wait_recv()

    class Spread:
        def __init__(self, n, at, first, ref, zs, zr, ys, yr, cs, cr, xs=None, xr=None):
            self.n, self.at, self.first, self.ref = n, at, first, ref
            self.zs, self.zr, self.ys, self.yr, self.cs, self.cr, self.xs, self.xr = zs, zr, ys, yr, cs, cr, xs, xr
            self.nx = X if xs is not None else 1

        def order(self, i):
            n = self.n
            return pick([sorted(range(n), key=lambda q: (abs(q - a), q))[i] for a in range(n)], self.at)

        def block(self, i, j, k, o):
            tps = lax.rem(y + Y - j, Y) * C + lax.rem(core + C - o, C)
            return self.ref(self.order(i), lax.rem(x + X - k, X), tps)

        def fan_y(self, i):
            piece = self.block(i, 0, 0, 0)
            return [(remote(piece, piece, self.ys.at[i, j - 1], self.yr.at[i, j - 1], to_y(j)), None)
                    for j in range(1, Y)]

        def fan_x(self, i, j):
            piece = self.block(i, j, 0, 0)
            return [(remote(piece, piece, self.xs.at[i, j, k - 1], self.xr.at[i, j, k - 1], to_x(k)), None)
                    for k in range(1, self.nx)]

        def fan_c(self, i, j, k):
            piece = self.block(i, j, k, 0)
            return [(remote(piece, piece, self.cs.at[i, j, k, o - 1], self.cr.at[i, j, k, o - 1], to_core(o)), None)
                    for o in range(1, C)]

        def fan(self, i):
            return self.fan_y(i) + self.fan_x(i, 0) + self.fan_c(i, 0, 0)

        def start_z(self, when=None, track=True):
            piece = self.block(0, 0, 0, 0)
            slot = self.zr.at[self.at]
            copies = []
            for sem, step in ((0, 1), (self.n, -1)):
                to = self.at + step
                copies.append((remote(piece, piece, self.zs.at[sem], slot, to_z(self.first + to)),
                               (to >= 0) & (to < self.n)))
            emit([], copies, when, track)

        def start(self):
            self.start_z()
            emit([], self.fan(0))

        def on_z(self, i, when=None, track=True):
            o = self.order(i)
            piece = self.block(i, 0, 0, 0)
            nxt = jnp.where(o < self.at, self.at + 1, self.at - 1)
            copy = remote(piece, piece, self.zs.at[i], self.zr.at[o], to_z(self.first + nxt))
            emit([copy], [(copy, (nxt >= 0) & (nxt < self.n))] + self.fan(i), when, track)

        def on_y(self, i, when=None, track=True):
            for j in range(1, Y):
                piece = self.block(i, j, 0, 0)
                wait = remote(piece, piece, self.ys.at[i, j - 1], self.yr.at[i, j - 1], to_y(j))
                emit([wait], self.fan_x(i, j) + self.fan_c(i, j, 0), when, track)

        def on_x(self, i):
            for j in range(Y):
                for k in range(1, self.nx):
                    arrived(self.block(i, j, k, 0), self.xs.at[i, j, k - 1], self.xr.at[i, j, k - 1])
                    emit([], self.fan_c(i, j, k))

        def on_c(self, i):
            for j in range(Y):
                for k in range(self.nx):
                    for o in range(1, C):
                        arrived(self.block(i, j, k, o), self.cs.at[i, j, k, o - 1], self.cr.at[i, j, k, o - 1])

    tok = Spread(G, g, base, lambda zi, xi, t: tok_g.at[rows_of(t, width), seq_at(zi)], t_zs, t_zr, t_ys, t_yr, t_cs, t_cr)
    mix = Spread(G, g, base, lambda zi, xi, t: mix_g.at[pl.ds(pl.multiple_of(t * ret + zi * hw, hw), hw)],
                 m_zs, m_zr, m_ys, m_yr, m_cs, m_cr)
    prj = Spread(Z, z, 0, lambda zi, xi, t: out_full.at[rows_of(zi * X + xi, rows), rows_of(t, ret)],
                 p_zs, p_zr, p_ys, p_yr, p_cs, p_cr, p_xs, p_xr)

    def place(w, owner):
        if w >= DOWN:
            return f_down.at[w - DOWN, rows_of(owner, rq)]
        ref = f_proj if w == 0 else f_up.at[w - 1]
        return ref.at[:, rows_of(owner, rows)] if strided else ref.at[owner]

    def mine(w, k):
        if w >= DOWN:
            return o_down.at[k, w - DOWN]
        return o_proj.at[k] if w == 0 else o_up.at[k, w - 1]

    def mul(ref, v):
        if strided:
            return nn(ref[...], v)
        total = nn(ref[0], v[0:rows, :])
        for f in range(1, n_fs):
            total += nn(ref[f], v[f * rows : (f + 1) * rows, :])
        return total

    locals_ = {}

    def z_send(w, when=None, track=True):
        copies = []
        for i in range(1, Z):
            to = prj.order(i)
            o = lax.rem(to + Z - z, Z) - 1
            copy = remote(mine(w, lax.rem(to, G)), place(w, me), wzs.at[w, o], wzr.at[w, o], to_z(to))
            copies.append((copy, None))
        emit([], copies, when, track)

    def x_own(w):
        for o in range(1, X):
            send(mine(w, g), place(w, me), wxs.at[w, 0, o - 1], wxr.at[w, 0, o - 1], to_x(o))
        copy = pltpu.make_async_copy(mine(w, g), place(w, me), local_sem.at[w])
        copy.start()
        locals_[w] = copy

    def relay(w, when=None, track=True):
        for k in range(1, Z):
            piece = place(w, lax.rem(z + Z - k, Z) * X + x)
            wait = remote(piece, piece, wzs.at[w, k - 1], wzr.at[w, k - 1], to_x(1) if X > 1 else to_core(1))
            emit([wait], [(remote(piece, piece, wxs.at[w, k, o - 1], wxr.at[w, k, o - 1], to_x(o)), None)
                          for o in range(1, X)], when, track)

    def finish(w):
        locals_[w].wait()
        for k in range(Z):
            for o in range(1, X):
                owner = lax.rem(z + Z - k, Z) * X + lax.rem(x + X - o, X)
                arrived(place(w, owner), wxs.at[w, k, o - 1], wxr.at[w, k, o - 1])

    def wide(col, n):
        return jnp.concatenate([col] * (n // LANES), axis=1) if n > LANES else col[:, :n]

    def column(row):
        return jnp.broadcast_to(row, (LANES, LANES)).T

    def columns(dst, row, n, count, first):
        w = part_of(n)
        per = n // w

        def one(f, carry):
            for r in range(per):
                c = column(scale_g[first + f, row + r : row + r + 1, :])[:w]
                if w % 8 == 0:
                    dst[pl.ds(pl.multiple_of((f * per + r) * w, 8), w), :] = c
                else:
                    dst[f * w : (f + 1) * w, :] = c
            return carry

        if w % 8 == 0:
            lax.fori_loop(0, count, one, 0, unroll=math.gcd(count, 4))
        else:
            for f in range(count):
                one(f, 0)

    loads[0].wait()
    scales[...] = jnp.zeros_like(scales)
    at = 0
    for ref in own_scales:
        n, w = ref.shape
        scales[at : at + n, :w] = ref[...]
        at += n
    scale_g[flat] = scales[...]
    pl.semaphore_wait(barrier, n_dev - 1)

    with jax.named_scope("start"):
        tok.start()

        def tell(o, carry):
            remote(scales, scale_g.at[flat], sc_s.at[o], sc_r.at[o], peer(o)).start()
            return carry

        lax.fori_loop(1, n_dev, tell, 0)

    ends = (z == 0) | (z == Z - 1)
    with jax.named_scope("cast"):
        for i in range(4):
            loads[1 + i].wait()
            t = st_proj[i].T
            for k in range(G):
                o_proj[k, i * hw : (i + 1) * hw, :] = t[k * hw : (k + 1) * hw, :].astype(BF)
        z_send(0, when=ends)
        x_own(0)
        loads[5].wait()
        own_out = out_full.at[rows_of(me, rows), rows_of(tp, ret)]
        o_out[...] = st_out[...].T.astype(BF)
        copy = pltpu.make_async_copy(o_out, own_out, local_sem.at[DOWN + Q])
        copy.start()
        copy.wait()
        prj.start_z(ends)
        loads[6].wait()
        loads[7].wait()

        def cast_up(k, carry):
            at = rows_of(k, chunk)
            t = st_up[:, at].T.astype(BF)
            for i in range(U):
                o_up[k, i] = t[i * uh : (i + 1) * uh]
            t = st_down[at, :].T.astype(BF)
            for i in range(Q):
                o_down[k, i] = t[i * rq : (i + 1) * rq]
            return carry

        lax.fori_loop(0, G, cast_up, 0)
        for w in range(1, DOWN + Q):
            x_own(w)

    with jax.named_scope("tables"):
        def gain_row(i, carry):
            gain_c[0, rows_of(i, LANES), :] = column(mix_gain[pl.ds(i, 1), :])
            gain_c[1, rows_of(i, LANES), :] = column(mlp_gain[pl.ds(i, 1), :])
            return carry

        lax.fori_loop(0, D // LANES, gain_row, 0, unroll=4)
        krow = lax.broadcasted_iota(jnp.int32, (L, L), 0)
        qcol = lax.broadcasted_iota(jnp.int32, (L, L), 1)
        dist = (qcol - krow).astype(F32)
        for h in range(hw // head):
            rate = forget[g * (hw // head) + h]
            decay[h] = jnp.where(dist >= 0.0, jnp.exp(-rate * jnp.maximum(dist, 0.0)), 0.0)

    with jax.named_scope("tok1"):
        tok.on_z(1)
        if G > 2:
            tok.on_z(2)
        z_send(0, when=jnp.logical_not(ends), track=False)
        tok.on_y(0)
    with jax.named_scope("scales"):
        def heard(o, carry):
            slot = scale_g.at[lax.rem(flat + n_dev - o, n_dev)]
            arrived(slot, sc_s.at[o], sc_r.at[o])
            return carry

        lax.fori_loop(1, n_dev, heard, 0)
        for i in range(4):
            columns(proj_c.at[i], i, ret // n_fs, n_fs, tp * n_fs)
    inner = jnp.logical_not(ends)
    with jax.named_scope("tok_y1"):
        tok.on_y(1)
    with jax.named_scope("relay0"):
        relay(0, when=ends)
        for w in range(1, DOWN):
            z_send(w, when=ends)
    with jax.named_scope("tok3"):
        for i in range(3, G):
            tok.on_z(i)
    with jax.named_scope("relay0b"):
        prj.start_z(inner, track=False)
        emit([], prj.fan(0))
        relay(0, when=inner, track=False)
        for k in range(1, min(Z, 3)):
            prj.on_z(k, when=inner)
    with jax.named_scope("finish0"):
        finish(0)

    tile = 256 if D % 256 == 0 else D
    r64 = lax.broadcasted_iota(jnp.int32, (head, head), 0)
    c64 = lax.broadcasted_iota(jnp.int32, (head, head), 1)
    odd = lax.rem(r64, 2) == 1
    swap = jnp.where((c64 == r64 - 1) & odd, 1.0, jnp.where((c64 == r64 + 1) & ~odd, -1.0, 0.0)).astype(BF)

    def turn(field):
        return field.astype(F32) * cos_t[...] + nn(swap, field) * sin_t[...]

    def attend(i):
        at = seq_at(tok.order(i))

        def add(t, square):
            v = tok_g[rows_of(t, tile), at].astype(F32)
            return square + jnp.sum(v * v, axis=0, keepdims=True)

        square = lax.fori_loop(0, D // tile, add, jnp.zeros((1, L), F32))
        factor = lax.rsqrt(square / D + 1e-6)

        def one(t, carry):
            here = rows_of(t, tile)
            normed[here, :] = (tok_g[here, at].astype(F32) * factor * wide(gain_c[0, here, :], L)).astype(BF)
            return carry

        lax.fori_loop(0, D // tile, one, 0)
        proj = mul(f_proj, normed[...])
        heads_at = pl.ds(pl.multiple_of(g * hw, hw), hw)
        q, k, v, gate = [
            (proj[n * hw : (n + 1) * hw, :] * wide(proj_c[n, heads_at, :], L)).astype(BF) for n in range(4)
        ]
        for h in range(hw // head):
            of = slice(h * head, (h + 1) * head)
            rot_q = turn(q[of]).astype(BF)
            rot_k = (turn(k[of]) * head ** (-0.5)).T.astype(BF)
            inner = (nn(rot_k, rot_q) * decay[h]).astype(BF)
            total = nn(v[of], inner)
            mean = jnp.sum(total * total, axis=0, keepdims=True) / head
            f = gate[of].astype(F32)
            value = f / (1.0 + jnp.exp(-f)) * (total * lax.rsqrt(mean + 0.01))
            mix_g[pl.ds(pl.multiple_of(tp * ret + g * hw + h * head, head), head), at] = value.astype(BF)

    with jax.named_scope("tok_y2"):
        for i in range(2, G - 1):
            tok.on_y(i)
    for i in range(G):
        if i == G - 1 and i > 1:
            with jax.named_scope("tok_y3"):
                tok.on_y(i, when=ends, track=False)
        with jax.named_scope("att%d" % i):
            tok.on_c(i)
            attend(i)
        if i == 0 and G > 2:
            with jax.named_scope("tok_y3"):
                tok.on_y(G - 1, when=inner)
        if i == min(1, G - 1):
            with jax.named_scope("prj_z0"):
                for k in range(3, Z):
                    prj.on_z(k, when=inner)
                for w in range(1, 1 + U // 2):
                    z_send(w, when=inner, track=False)
        if i == G - 2:
            with jax.named_scope("prj_y0"):
                prj.on_y(0)
    with jax.named_scope("mix_start"):
        mix.start()
    with jax.named_scope("prj_y12"):
        for k in range(1, min(Z, 3)):
            prj.on_y(k, when=inner)
    with jax.named_scope("prj_z"):
        for k in range(1, min(Z, 3)):
            prj.on_z(k, when=ends, track=False)
        for k in range(3, Z):
            prj.on_z(k, when=ends, track=False)
    with jax.named_scope("mix_z"):
        for i in range(1, min(G, 3)):
            mix.on_z(i)
    with jax.named_scope("prj_y1"):
        for k in range(1, min(Z, 3)):
            prj.on_y(k, when=ends, track=False)
    with jax.named_scope("mix_z3"):
        for i in range(3, G):
            mix.on_z(i)
    for w in range(DOWN, DOWN + Q):
        z_send(w, when=ends)
    with jax.named_scope("prj_y3"):
        for k in range(3, Z):
            prj.on_y(k)
    with jax.named_scope("columns"):
        columns(out_c, 4, D // n_dev, n_dev, 0)
        columns(down_c, 5, width // n_fs, n_fs, tp * n_fs)
        columns(up_c, 6, G * chunk // n_fs, n_fs, tp * n_fs)
    with jax.named_scope("relay1"):
        for w in range(1, 1 + U // 2):
            relay(w)
    with jax.named_scope("mix_y"):
        for i in range(G):
            mix.on_y(i)
            if i == 1:
                for w in range(1 + U // 2, DOWN + Q):
                    z_send(w, when=inner, track=False)
    with jax.named_scope("prj_x"):
        for k in range(Z):
            prj.on_x(k)
    with jax.named_scope("prj_c"):
        for k in range(Z):
            prj.on_c(k)
    with jax.named_scope("mix_c"):
        for i in range(G):
            mix.on_c(i)

    tb = cfg.tb
    n_blocks = G * L // tb

    def settle(n):
        b = n * C + core
        at = rows_of(b, tb)
        v = nn(out_full[...], mix_g[:, at]) * wide(out_c[...], tb)
        a = (tok_g[:, at].astype(F32) + v).astype(BF).astype(F32)
        factor = lax.rsqrt(jnp.sum(a * a, axis=0, keepdims=True) / D + 1e-6)
        after[b] = (a * factor * wide(gain_c[1], tb)).astype(BF)
        for o in range(1, C):
            send(after.at[b], after.at[b], ncs.at[n, o - 1], ncr.at[n, o - 1], to_core(o))

    def settled(n):
        for o in range(1, C):
            arrived(after.at[n * C + lax.rem(core + C - o, C)], ncs.at[n, o - 1], ncr.at[n, o - 1])

    def expand(b, carry):
        at = rows_of(b, tb)
        for i in range(U):
            sc = wide(up_c[pl.ds(pl.multiple_of(g * chunk + i * uh, uh), uh), :], tb)
            u = jnp.maximum(mul(f_up.at[i], after[b]) * sc, 0.0)
            hidden[i * uh : (i + 1) * uh, at] = (u * u).astype(BF)
        return carry

    wt = width // Q
    ppt = n_fs // n_tp

    def shrink(q):
        def one(b, carry):
            at = rows_of(b, tb)
            parts[q, :, at] = nn(f_down[q], hidden[:, at]).astype(BF)
            return carry

        lax.fori_loop(0, G * L // tb, one, 0)
        for o in range(1, C):
            for j in range(Y):
                send(parts.at[q, rows_of(j * C + lax.rem(core + o, C), wt)], core_in.at[q, o - 1, j],
                     rcs.at[q, o - 1, j], rcr.at[q, o - 1, j], to_core(o))

    def reduce_core(q):
        for o in range(1, C):
            for j in range(Y):
                arrived(core_in.at[q, o - 1, j], rcs.at[q, o - 1, j], rcr.at[q, o - 1, j])
        for n in range(Y - 1, -1, -1):
            j = lax.rem(y + n, Y)
            value = parts[q, rows_of(j * C + core, wt), :].astype(F32)
            for o in range(1, C):
                value += core_in[q, o - 1, j].astype(F32)
            y_out[q, j] = value.astype(BF)
            if n:
                send(y_out.at[q, j], y_in.at[q, n - 1], rys.at[q, n - 1], ryr.at[q, n - 1], to_y(n))

    def reduce_y(q):
        value = y_out[q, y].astype(F32)
        for j in range(1, Y):
            arrived(y_in.at[q, j - 1], rys.at[q, j - 1], ryr.at[q, j - 1])
            value += y_in[q, j - 1].astype(F32)
        z_out[q] = value.astype(BF)
        for i in range(G - 1, 0, -1):
            s = tok.order(i)
            send(z_out.at[q, :, seq_at(s)], z_in.at[q, g], rzs.at[q, i], rzr.at[q, g], to_z(base + s))

    def reduce_z(q):
        total = z_out[q, :, seq_at(g)].astype(F32)
        for i in range(1, G):
            o = tok.order(i)
            arrived(z_in.at[q, o], rzs.at[q, i], rzr.at[q, o])
            total += z_in[q, o].astype(F32)
        for h in range(ppt):
            here = slice(h * rows + q * rq, h * rows + (q + 1) * rq)
            t = total[h * rq : (h + 1) * rq] * wide(down_c[here, :], L)
            out_ref[here, :] = (keep[here, :].astype(F32) + t).astype(BF)

    for n in range(n_blocks // C):
        with jax.named_scope("settle%d" % n):
            settle(n)
            if n == 0:
                for w in range(1 + U // 2, DOWN):
                    relay(w)
    with jax.named_scope("keep"):
        mine_at = rows_of(tp, width)
        v = nn(out_full[mine_at, :], mix_g[:, seq_at(g)]) * wide(out_c[mine_at, :], L)
        keep[...] = (tok_g[mine_at, seq_at(g)].astype(F32) + v).astype(BF)
    with jax.named_scope("finish1"):
        for w in range(1, 1 + U):
            finish(w)
    with jax.named_scope("expand"):
        for n in range(n_blocks // C):
            settled(n)
        relay(DOWN)
        lax.fori_loop(0, n_blocks, expand, 0)
    for n in range(Q + 1):
        with jax.named_scope("down%d" % n):
            if n < Q:
                with jax.named_scope("drel"):
                    for w in range(n + 1, Q if n == 1 else n + 2):
                        if w < Q and n < 2:
                            relay(DOWN + w)
                with jax.named_scope("dfin"):
                    finish(DOWN + n)
                with jax.named_scope("shrink"):
                    shrink(n)
                with jax.named_scope("rcore"):
                    reduce_core(n)
            if n:
                with jax.named_scope("ry"):
                    reduce_y(n - 1)
    with jax.named_scope("final"):
        for q in range(Q):
            reduce_z(q)
    for copy, when in pending:
        if when is None:
            copy.wait_send()
        else:
            pl.when(when)(copy.wait_send)

    def told(o, carry):
        remote(scales, scale_g.at[flat], sc_s.at[o], sc_r.at[o], peer(o)).wait_send()
        return carry

    lax.fori_loop(1, n_dev, told, 0)


def tables(length, head):
    half = head // 2
    inverse = 1.0 / 10000.0 ** np.linspace(0.0, 1.0, half)
    angle = np.arange(length)[:, None] * inverse.astype(np.float32).astype(np.float64)[None, :]
    spread = lambda a: np.repeat(a, 2, axis=1).T.astype(np.float32)
    return spread(np.cos(angle)), spread(np.sin(angle))


def solution(mesh):
    n_fs, n_tp = mesh.shape["fs"], mesh.shape["tp"]
    heights = [getattr(d, "coords", (0, 0, i))[2] for i, d in enumerate(mesh.devices[:, 0])]
    X = heights.count(heights[0])
    if n_fs % X:
        X = 1
    Z = n_fs // X
    cores = [getattr(d, "core_on_chip", 0) for d in mesh.devices[0]]
    C = len(set(cores))
    if n_tp % C:
        C = 1
    Y = n_tp // C

    def on_device(tokens, mix_gain, mlp_gain, wq, wk, wv, wg, wo, wu, wd, sq, sk, sv, sg, so, su, sd, forget):
        cfg = Cfg()
        cfg.Z, cfg.X, cfg.Y, cfg.C = Z, X, Y, C
        width, L = tokens.shape
        cfg.width, cfg.L, cfg.D = width, L, width * n_tp
        D = cfg.D
        heads = forget.shape[0]
        G = cfg.G = next(q for q in (4, 2, 1) if Z % q == 0 and heads % q == 0)
        ret = cfg.ret = wq.shape[1]
        cfg.head = ret // heads
        hw = cfg.hw = ret // G
        chunk = cfg.chunk = wu.shape[1] // G
        rows = cfg.rows = wq.shape[0]
        n_dev = n_fs * n_tp
        Q = cfg.Q = 4 if rows % 64 == 0 else 1
        U = cfg.U = 2
        scales = [scale_rows(s) for s in (sq, sk, sv, sg, so, sd, su)]
        n_rows = -(-sum(s.shape[0] for s in scales) // 8) * 8
        gains = [v.reshape(-1, LANES) for v in (mix_gain, mlp_gain)]
        cos_t, sin_t = tables(L, cfg.head)
        vm = pl.BlockSpec(memory_space=pltpu.VMEM)
        hbm = pl.BlockSpec(memory_space=pl.ANY)
        dma = pltpu.SemaphoreType.DMA
        strided = rows % LANES == 0
        vmem = lambda *shape, t=BF: pltpu.VMEM(shape, t)
        stack = (lambda *n: vmem(*n, D)) if strided else (lambda *n: vmem(*n[:-1], n_fs, n[-1], rows))
        wt = width // Q
        tb = cfg.tb = 256 if G * L % (256 * C) == 0 else LANES
        scratch = [
            vmem(D, G * L), vmem(ret * n_tp, G * L), vmem(D, ret * n_tp), stack(4 * hw), stack(U, chunk // U),
            vmem(Q, D // Q, chunk), vmem(G, 4 * hw, rows), vmem(G, U, chunk // U, rows), vmem(G, Q, rows // Q, chunk),
            vmem(rows, ret),
            vmem(4, rows, ret, t=F32), vmem(*wo.shape, t=F32), vmem(*wu.shape, t=F32), vmem(*wd.shape, t=F32),
            vmem(Q, D // Q, G * L), vmem(Q, max(C - 1, 1), Y, wt, G * L), vmem(Q, Y, wt, G * L),
            vmem(Q, max(Y - 1, 1), wt, G * L), vmem(Q, wt, G * L), vmem(Q, G, wt, L),
            vmem(G * L // tb, D, tb), vmem(D, L), vmem(chunk, G * L), vmem(width, L),
            vmem(2, D, LANES, t=F32), vmem(D, LANES, t=F32), vmem(G * chunk, LANES, t=F32),
            vmem(width, LANES, t=F32), vmem(4, ret, LANES, t=F32), vmem(hw // cfg.head, L, L, t=F32),
            vmem(n_dev, n_rows, LANES, t=F32), dma((8,)), dma((2 + U + Q,)),
        ]
        line = lambda n, nx: [(n + 1,), (n,), (n, Y), (n, Y), (n, Y, nx, C), (n, Y, nx, C)]
        W = 1 + U + Q
        shapes = [(n_dev,), (n_dev,), (W, Z), (W, Z), (W, Z, X), (W, Z, X)] + line(G, 1) + line(G, 1)
        first = line(Z, X)
        shapes += first[:4] + [(Z, Y, X), (Z, Y, X)] + first[4:]
        shapes += [(Q, C, Y), (Q, C, Y), (Q, Y), (Q, Y), (Q, G), (Q, G)]
        shapes += [(G * L // tb, C), (G * L // tb, C)]
        scratch += [dma(s) for s in shapes] + [vmem(n_rows, LANES, t=F32)]
        return pl.pallas_call(
            functools.partial(kernel, cfg),
            out_shape=jax.ShapeDtypeStruct((width, L), BF),
            in_specs=[hbm] + [vm] * 4 + [pl.BlockSpec(memory_space=pltpu.SMEM)] + [hbm] * 7 + [vm] * 7,
            out_specs=vm,
            scratch_shapes=scratch,
            compiler_params=pltpu.CompilerParams(
                collective_id=0, has_side_effects=True, vmem_limit_bytes=63 * 2**20
            ),
            name="layer",
        )(tokens, *gains, jnp.asarray(cos_t), jnp.asarray(sin_t), forget, wq, wk, wv, wg, wo, wu, wd, *scales)

    cut = P(("tp", "fs"))
    rows, cols = P("fs", "tp"), P("tp", "fs")
    in_specs = (cols, P(), P(), rows, rows, rows, rows, cols, rows, cols) + (cut,) * 7 + (P("tp"),)
    return jax.shard_map(on_device, mesh=mesh, in_specs=in_specs, out_specs=cols, check_vma=False)
```

```python
import functools
import math

import jax
import jax.numpy as jnp
import numpy as np
from jax import lax
from jax.experimental import pallas as pl
from jax.experimental.pallas import tpu as pltpu
from jax.sharding import PartitionSpec as P

MESH = pl.DeviceIdType.MESH
BF = jnp.bfloat16
F32 = jnp.float32
LANES = 128


def nn(a, b):
    return lax.dot_general(a, b, (((1,), (0,)), ((), ())), preferred_element_type=F32)


def pick(table, at):
    value = jnp.int32(table[0])
    for a in range(1, len(table)):
        value = jnp.where(at == a, jnp.int32(table[a]), value)
    return value


def part_of(n):
    return min(n, LANES)


def scale_rows(s):
    n = s.shape[0]
    return s.reshape(-1, part_of(n))


class Cfg:
    pass


def kernel(cfg, *refs):
    Z, X, Y, C, G = cfg.Z, cfg.X, cfg.Y, cfg.C, cfg.G
    n_tp, n_fs = Y * C, Z * X
    n_dev = n_tp * n_fs
    L, width, D, ret, hw, chunk, rows = cfg.L, cfg.width, cfg.D, cfg.ret, cfg.hw, cfg.chunk, cfg.rows
    head, Q, U = cfg.head, cfg.Q, cfg.U
    rq, uh = rows // Q, chunk // U
    DOWN = 1 + U
    (tokens, mix_gain, mlp_gain, cos_t, sin_t, forget, wq, wk, wv, wg, wo, wu, wd) = refs[:13]
    own_scales, out_ref = refs[13:20], refs[20]
    (tok_g, mix_g, out_full, f_proj, f_up, f_down, o_proj, o_up, o_down, o_out, st_proj, st_out, st_up, st_down,
     parts, core_in, y_out, y_in, z_out, z_in, after, normed, hidden, keep, gain_c, out_c, up_c, down_c, proj_c,
     decay, scale_g, load_sem, local_sem, sc_s, sc_r, wzs, wzr, wxs, wxr,
     t_zs, t_zr, t_ys, t_yr, t_cs, t_cr, m_zs, m_zr, m_ys, m_yr, m_cs, m_cr,
     p_zs, p_zr, p_ys, p_yr, p_xs, p_xr, p_cs, p_cr, rcs, rcr, rys, ryr, rzs, rzr, ncs, ncr, scales) = refs[21:]
    me = lax.axis_index("fs")
    tp = lax.axis_index("tp")
    z = me // X
    x = lax.rem(me, X)
    y = tp // C
    core = lax.rem(tp, C)
    flat = tp * n_fs + me
    g = lax.rem(z, G)
    base = z - g
    strided = rows % LANES == 0

    def to_z(zz):
        return {"fs": zz * X + x}

    def to_x(o):
        return {"fs": z * X + lax.rem(x + o, X)}

    def to_y(o):
        return {"tp": lax.rem(y + o, Y) * C + core}

    def to_core(o):
        return {"tp": y * C + lax.rem(core + o, C)}

    def peer(o):
        q = lax.rem(flat + o, n_dev)
        return {"fs": lax.rem(q, n_fs), "tp": q // n_fs}

    barrier = pltpu.get_barrier_semaphore()

    def greet(o, carry):
        pl.semaphore_signal(barrier, inc=1, device_id=peer(o), device_id_type=MESH)
        return carry

    lax.fori_loop(1, n_dev, greet, 0)

    def rows_of(i, n):
        return pl.ds(pl.multiple_of(i * n, n), n)

    def seq_at(s):
        return pl.ds(pl.multiple_of(s * L, LANES), L)

    own_tok = tok_g.at[rows_of(tp, width), seq_at(g)]
    loads = [(tokens, own_tok)]
    loads += [(w, st_proj.at[i]) for i, w in enumerate((wq, wk, wv, wg))]
    loads += [(wo, st_out), (wu, st_up), (wd, st_down)]
    loads = [pltpu.make_async_copy(a, b, load_sem.at[i]) for i, (a, b) in enumerate(loads)]
    for copy in loads:
        copy.start()

    pending = []

    def remote(src, dst, ss, rs, where):
        return pltpu.make_async_remote_copy(
            src_ref=src, dst_ref=dst, send_sem=ss, recv_sem=rs, device_id=where, device_id_type=MESH
        )

    def emit(waits, copies, when=None, track=True):
        def go():
            for copy in waits:
                copy.wait_recv()
            for copy, ok in copies:
                if ok is None:
                    copy.start()
                else:
                    pl.when(ok)(copy.start)

        if when is None:
            go()
        else:
            pl.when(when)(go)
        if track:
            pending.extend(copies)

    def send(*a):
        emit([], [(remote(*a), None)])

    def arrived(ref, ss, rs):
        remote(ref, ref, ss, rs, to_core(1) if C > 1 else to_z(z)).wait_recv()

    class Spread:
        def __init__(self, n, at, first, ref, zs, zr, ys, yr, cs, cr, xs=None, xr=None):
            self.n, self.at, self.first, self.ref = n, at, first, ref
            self.zs, self.zr, self.ys, self.yr, self.cs, self.cr, self.xs, self.xr = zs, zr, ys, yr, cs, cr, xs, xr
            self.nx = X if xs is not None else 1

        def order(self, i):
            n = self.n
            return pick([sorted(range(n), key=lambda q: (abs(q - a), q))[i] for a in range(n)], self.at)

        def block(self, i, j, k, o):
            tps = lax.rem(y + Y - j, Y) * C + lax.rem(core + C - o, C)
            return self.ref(self.order(i), lax.rem(x + X - k, X), tps)

        def fan_y(self, i):
            piece = self.block(i, 0, 0, 0)
            return [(remote(piece, piece, self.ys.at[i, j - 1], self.yr.at[i, j - 1], to_y(j)), None)
                    for j in range(1, Y)]

        def fan_x(self, i, j):
            piece = self.block(i, j, 0, 0)
            return [(remote(piece, piece, self.xs.at[i, j, k - 1], self.xr.at[i, j, k - 1], to_x(k)), None)
                    for k in range(1, self.nx)]

        def fan_c(self, i, j, k):
            piece = self.block(i, j, k, 0)
            return [(remote(piece, piece, self.cs.at[i, j, k, o - 1], self.cr.at[i, j, k, o - 1], to_core(o)), None)
                    for o in range(1, C)]

        def fan(self, i):
            return self.fan_y(i) + self.fan_x(i, 0) + self.fan_c(i, 0, 0)

        def start_z(self, when=None, track=True):
            piece = self.block(0, 0, 0, 0)
            slot = self.zr.at[self.at]
            copies = []
            for sem, step in ((0, 1), (self.n, -1)):
                to = self.at + step
                copies.append((remote(piece, piece, self.zs.at[sem], slot, to_z(self.first + to)),
                               (to >= 0) & (to < self.n)))
            emit([], copies, when, track)

        def start(self):
            self.start_z()
            emit([], self.fan(0))

        def on_z(self, i, when=None, track=True):
            o = self.order(i)
            piece = self.block(i, 0, 0, 0)
            nxt = jnp.where(o < self.at, self.at + 1, self.at - 1)
            copy = remote(piece, piece, self.zs.at[i], self.zr.at[o], to_z(self.first + nxt))
            emit([copy], [(copy, (nxt >= 0) & (nxt < self.n))] + self.fan(i), when, track)

        def on_y(self, i, when=None, track=True):
            for j in range(1, Y):
                piece = self.block(i, j, 0, 0)
                wait = remote(piece, piece, self.ys.at[i, j - 1], self.yr.at[i, j - 1], to_y(j))
                emit([wait], self.fan_x(i, j) + self.fan_c(i, j, 0), when, track)

        def on_x(self, i):
            for j in range(Y):
                for k in range(1, self.nx):
                    arrived(self.block(i, j, k, 0), self.xs.at[i, j, k - 1], self.xr.at[i, j, k - 1])
                    emit([], self.fan_c(i, j, k))

        def on_c(self, i):
            for j in range(Y):
                for k in range(self.nx):
                    for o in range(1, C):
                        arrived(self.block(i, j, k, o), self.cs.at[i, j, k, o - 1], self.cr.at[i, j, k, o - 1])

    tok = Spread(G, g, base, lambda zi, xi, t: tok_g.at[rows_of(t, width), seq_at(zi)], t_zs, t_zr, t_ys, t_yr, t_cs, t_cr)
    mix = Spread(G, g, base, lambda zi, xi, t: mix_g.at[pl.ds(pl.multiple_of(t * ret + zi * hw, hw), hw)],
                 m_zs, m_zr, m_ys, m_yr, m_cs, m_cr)
    prj = Spread(Z, z, 0, lambda zi, xi, t: out_full.at[rows_of(zi * X + xi, rows), rows_of(t, ret)],
                 p_zs, p_zr, p_ys, p_yr, p_cs, p_cr, p_xs, p_xr)

    def place(w, owner):
        if w >= DOWN:
            return f_down.at[w - DOWN, rows_of(owner, rq)]
        ref = f_proj if w == 0 else f_up.at[w - 1]
        return ref.at[:, rows_of(owner, rows)] if strided else ref.at[owner]

    def mine(w, k):
        if w >= DOWN:
            return o_down.at[k, w - DOWN]
        return o_proj.at[k] if w == 0 else o_up.at[k, w - 1]

    def mul(ref, v):
        if strided:
            return nn(ref[...], v)
        total = nn(ref[0], v[0:rows, :])
        for f in range(1, n_fs):
            total += nn(ref[f], v[f * rows : (f + 1) * rows, :])
        return total

    locals_ = {}

    def z_send(w, when=None, track=True, ends_too=None):
        copies = []
        for i in range(1, Z):
            to = prj.order(i)
            o = lax.rem(to + Z - z, Z) - 1
            copy = remote(mine(w, lax.rem(to, G)), place(w, me), wzs.at[w, o], wzr.at[w, o], to_z(to))
            ok = None
            if ends_too is not None:
                ok = (to == 0) | (to == Z - 1)
                ok = ok if ends_too else jnp.logical_not(ok)
            copies.append((copy, ok))
        emit([], copies, when, track)

    def from_x(w):
        n = Z * (X - 1)
        if w >= DOWN:
            return f_down.at[w - DOWN, pl.ds(0, n * rq)]
        ref = f_proj if w == 0 else f_up.at[w - 1]
        return ref.at[:, pl.ds(0, n * rows)] if strided else ref.at[pl.ds(0, n)]

    def x_own(w):
        for o in range(1, X):
            remote(mine(w, g), place(w, me), wxs.at[w], wxr.at[w], to_x(o)).start()
        copy = pltpu.make_async_copy(mine(w, g), place(w, me), local_sem.at[w])
        copy.start()
        locals_[w] = copy

    def relay(w, when=None, track=True):
        for k in range(1, Z):
            piece = place(w, lax.rem(z + Z - k, Z) * X + x)
            wait = remote(piece, piece, wzs.at[w, k - 1], wzr.at[w, k - 1], to_x(1) if X > 1 else to_core(1))
            emit([wait], [(remote(piece, piece, wxs.at[w], wxr.at[w], to_x(o)), None) for o in range(1, X)],
                 when, False)

    def finish(w):
        locals_[w].wait()
        arrived(from_x(w), wxs.at[w], wxr.at[w])

    def wide(col, n):
        return jnp.concatenate([col] * (n // LANES), axis=1) if n > LANES else col[:, :n]

    def column(row):
        return jnp.broadcast_to(row, (LANES, LANES)).T

    def columns(dst, row, n, count, first):
        w = part_of(n)
        per = n // w

        def one(f, carry):
            for r in range(per):
                c = column(scale_g[first + f, row + r : row + r + 1, :])[:w]
                if w % 8 == 0:
                    dst[pl.ds(pl.multiple_of((f * per + r) * w, 8), w), :] = c
                else:
                    dst[f * w : (f + 1) * w, :] = c
            return carry

        if w % 8 == 0:
            lax.fori_loop(0, count, one, 0, unroll=math.gcd(count, 4))
        else:
            for f in range(count):
                one(f, 0)

    loads[0].wait()
    scales[...] = jnp.zeros_like(scales)
    at = 0
    for ref in own_scales:
        n, w = ref.shape
        scales[at : at + n, :w] = ref[...]
        at += n
    scale_g[flat] = scales[...]
    pl.semaphore_wait(barrier, n_dev - 1)

    with jax.named_scope("start"):
        tok.start()

        def tell(o, carry):
            remote(scales, scale_g.at[flat], sc_s.at[0], sc_r.at[0], peer(o)).start()
            return carry

        lax.fori_loop(1, n_dev, tell, 0)

    ends = (z == 0) | (z == Z - 1)
    with jax.named_scope("cast"):
        for i in range(4):
            loads[1 + i].wait()
            t = st_proj[i].T
            for k in range(G):
                o_proj[k, i * hw : (i + 1) * hw, :] = t[k * hw : (k + 1) * hw, :].astype(BF)
        z_send(0, when=ends)
        x_own(0)
        loads[5].wait()
        own_out = out_full.at[rows_of(me, rows), rows_of(tp, ret)]
        o_out[...] = st_out[...].T.astype(BF)
        copy = pltpu.make_async_copy(o_out, own_out, local_sem.at[DOWN + Q])
        copy.start()
        copy.wait()
        prj.start_z(ends)
        loads[6].wait()
        loads[7].wait()

        def cast_up(k, carry):
            at = rows_of(k, chunk)
            t = st_up[:, at].T.astype(BF)
            for i in range(U):
                o_up[k, i] = t[i * uh : (i + 1) * uh]
            t = st_down[at, :].T.astype(BF)
            for i in range(Q):
                o_down[k, i] = t[i * rq : (i + 1) * rq]
            return carry

        lax.fori_loop(0, G, cast_up, 0)
        for w in range(1, DOWN + Q):
            x_own(w)

    with jax.named_scope("tables"):
        def gain_row(i, carry):
            gain_c[0, rows_of(i, LANES), :] = column(mix_gain[pl.ds(i, 1), :])
            gain_c[1, rows_of(i, LANES), :] = column(mlp_gain[pl.ds(i, 1), :])
            return carry

        lax.fori_loop(0, D // LANES, gain_row, 0, unroll=4)
        krow = lax.broadcasted_iota(jnp.int32, (L, L), 0)
        qcol = lax.broadcasted_iota(jnp.int32, (L, L), 1)
        dist = (qcol - krow).astype(F32)
        for h in range(hw // head):
            rate = forget[g * (hw // head) + h]
            decay[h] = jnp.where(dist >= 0.0, jnp.exp(-rate * jnp.maximum(dist, 0.0)), 0.0)

    with jax.named_scope("tok1"):
        tok.on_z(1)
        if G > 2:
            tok.on_z(2)
        z_send(0, when=jnp.logical_not(ends), track=False)
        tok.on_y(0)
    with jax.named_scope("scales"):
        others = scale_g.at[pl.ds(0, n_dev - 1)]
        arrived(others, sc_s.at[0], sc_r.at[0])
        for i in range(4):
            columns(proj_c.at[i], i, ret // n_fs, n_fs, tp * n_fs)
    with jax.named_scope("columns"):
        columns(out_c, 4, D // n_dev, n_dev, 0)
        columns(down_c, 5, width // n_fs, n_fs, tp * n_fs)
        columns(up_c, 6, G * chunk // n_fs, n_fs, tp * n_fs)
    inner = jnp.logical_not(ends)
    with jax.named_scope("tok_y1"):
        tok.on_y(1)
    with jax.named_scope("relay0"):
        relay(0, when=ends)
        for w in range(1, DOWN):
            z_send(w, when=ends)
    with jax.named_scope("tok3"):
        for i in range(3, G):
            tok.on_z(i)
    with jax.named_scope("relay0b"):
        prj.start_z(inner, track=False)
        emit([], prj.fan(0))
        relay(0, when=inner, track=False)
        for k in range(1, min(Z, 3)):
            prj.on_z(k, when=inner)
    with jax.named_scope("finish0"):
        finish(0)

    tile = 256 if D % 256 == 0 else D
    r64 = lax.broadcasted_iota(jnp.int32, (head, head), 0)
    c64 = lax.broadcasted_iota(jnp.int32, (head, head), 1)
    odd = lax.rem(r64, 2) == 1
    swap = jnp.where((c64 == r64 - 1) & odd, 1.0, jnp.where((c64 == r64 + 1) & ~odd, -1.0, 0.0)).astype(BF)

    def turn(field):
        return field.astype(F32) * cos_t[...] + nn(swap, field) * sin_t[...]

    def attend(i):
        at = seq_at(tok.order(i))

        def add(t, square):
            v = tok_g[rows_of(t, tile), at].astype(F32)
            return square + jnp.sum(v * v, axis=0, keepdims=True)

        square = lax.fori_loop(0, D // tile, add, jnp.zeros((1, L), F32))
        factor = lax.rsqrt(square / D + 1e-6)

        def one(t, carry):
            here = rows_of(t, tile)
            normed[here, :] = (tok_g[here, at].astype(F32) * factor * wide(gain_c[0, here, :], L)).astype(BF)
            return carry

        lax.fori_loop(0, D // tile, one, 0)
        proj = mul(f_proj, normed[...])
        heads_at = pl.ds(pl.multiple_of(g * hw, hw), hw)
        q, k, v, gate = [
            (proj[n * hw : (n + 1) * hw, :] * wide(proj_c[n, heads_at, :], L)).astype(BF) for n in range(4)
        ]
        for h in range(hw // head):
            of = slice(h * head, (h + 1) * head)
            rot_q = turn(q[of]).astype(BF)
            rot_k = (turn(k[of]) * head ** (-0.5)).T.astype(BF)
            inner = (nn(rot_k, rot_q) * decay[h]).astype(BF)
            total = nn(v[of], inner)
            mean = jnp.sum(total * total, axis=0, keepdims=True) / head
            f = gate[of].astype(F32)
            value = f / (1.0 + jnp.exp(-f)) * (total * lax.rsqrt(mean + 0.01))
            mix_g[pl.ds(pl.multiple_of(tp * ret + g * hw + h * head, head), head), at] = value.astype(BF)

    with jax.named_scope("tok_y2"):
        for i in range(2, G - 1):
            tok.on_y(i)
    for i in range(G):
        if i == G - 1 and i > 1:
            with jax.named_scope("tok_y3"):
                tok.on_y(i, when=ends, track=False)
        with jax.named_scope("att%d" % i):
            tok.on_c(i)
            attend(i)
        if i == 0 and G > 2:
            with jax.named_scope("tok_y3"):
                tok.on_y(G - 1, when=inner)
        if i == min(1, G - 1):
            with jax.named_scope("prj_z0"):
                for k in range(3, Z):
                    prj.on_z(k, when=inner)
                for w in range(1, 1 + U // 2):
                    z_send(w, when=inner, track=False)
        if i == G - 2:
            with jax.named_scope("prj_y0"):
                prj.on_y(0)
    with jax.named_scope("mix_start"):
        mix.start()
    with jax.named_scope("prj_y12"):
        for k in range(1, min(Z, 3)):
            prj.on_y(k, when=inner)
    with jax.named_scope("prj_z"):
        for k in range(1, min(Z, 3)):
            prj.on_z(k, when=ends, track=False)
        for k in range(3, Z):
            prj.on_z(k, when=ends, track=False)
    with jax.named_scope("mix_z"):
        for i in range(1, min(G, 3)):
            mix.on_z(i)
    with jax.named_scope("prj_y1"):
        for k in range(1, min(Z, 3)):
            prj.on_y(k, when=ends, track=False)
    with jax.named_scope("mix_z3"):
        for i in range(3, G):
            mix.on_z(i)
    for w in range(DOWN, DOWN + Q):
        z_send(w, when=ends)
    with jax.named_scope("prj_y3"):
        for k in range(3, Z):
            prj.on_y(k)
    with jax.named_scope("relay1"):
        for w in range(1, 1 + U // 2):
            relay(w)
    with jax.named_scope("mix_y"):
        for i in range(G):
            mix.on_y(i)
            if i == 1:
                for w in range(1 + U // 2, DOWN + Q):
                    z_send(w, when=inner, track=False)
    with jax.named_scope("prj_x"):
        for k in range(Z):
            prj.on_x(k)
    with jax.named_scope("prj_c"):
        for k in range(Z):
            prj.on_c(k)
    with jax.named_scope("mix_c"):
        for i in range(G):
            mix.on_c(i)

    tb = cfg.tb
    n_blocks = G * L // tb

    def settle(n):
        b = n * C + core
        at = rows_of(b, tb)
        v = nn(out_full[...], mix_g[:, at]) * wide(out_c[...], tb)
        a = (tok_g[:, at].astype(F32) + v).astype(BF).astype(F32)
        factor = lax.rsqrt(jnp.sum(a * a, axis=0, keepdims=True) / D + 1e-6)
        after[b] = (a * factor * wide(gain_c[1], tb)).astype(BF)
        for o in range(1, C):
            send(after.at[b], after.at[b], ncs.at[n, o - 1], ncr.at[n, o - 1], to_core(o))

    def settled(n):
        for o in range(1, C):
            arrived(after.at[n * C + lax.rem(core + C - o, C)], ncs.at[n, o - 1], ncr.at[n, o - 1])

    def expand(b, carry):
        at = rows_of(b, tb)
        for i in range(U):
            sc = wide(up_c[pl.ds(pl.multiple_of(g * chunk + i * uh, uh), uh), :], tb)
            u = jnp.maximum(mul(f_up.at[i], after[b]) * sc, 0.0)
            hidden[i * uh : (i + 1) * uh, at] = (u * u).astype(BF)
        return carry

    wt = width // Q
    ppt = n_fs // n_tp

    def shrink(q):
        def one(b, carry):
            at = rows_of(b, tb)
            parts[q, :, at] = nn(f_down[q], hidden[:, at]).astype(BF)
            return carry

        lax.fori_loop(0, G * L // tb, one, 0)
        for o in range(1, C):
            for j in range(Y):
                send(parts.at[q, rows_of(j * C + lax.rem(core + o, C), wt)], core_in.at[q, o - 1, j],
                     rcs.at[q, o - 1, j], rcr.at[q, o - 1, j], to_core(o))

    def reduce_core(q):
        for o in range(1, C):
            for j in range(Y):
                arrived(core_in.at[q, o - 1, j], rcs.at[q, o - 1, j], rcr.at[q, o - 1, j])
        for n in range(Y - 1, -1, -1):
            j = lax.rem(y + n, Y)
            value = parts[q, rows_of(j * C + core, wt), :].astype(F32)
            for o in range(1, C):
                value += core_in[q, o - 1, j].astype(F32)
            y_out[q, j] = value.astype(BF)
            if n:
                send(y_out.at[q, j], y_in.at[q, n - 1], rys.at[q, n - 1], ryr.at[q, n - 1], to_y(n))

    def reduce_y(q):
        value = y_out[q, y].astype(F32)
        for j in range(1, Y):
            arrived(y_in.at[q, j - 1], rys.at[q, j - 1], ryr.at[q, j - 1])
            value += y_in[q, j - 1].astype(F32)
        z_out[q] = value.astype(BF)
        for i in range(G - 1, 0, -1):
            s = tok.order(i)
            send(z_out.at[q, :, seq_at(s)], z_in.at[q, g], rzs.at[q, i], rzr.at[q, g], to_z(base + s))

    def reduce_z(q):
        total = z_out[q, :, seq_at(g)].astype(F32)
        for i in range(1, G):
            o = tok.order(i)
            arrived(z_in.at[q, o], rzs.at[q, i], rzr.at[q, o])
            total += z_in[q, o].astype(F32)
        for h in range(ppt):
            here = slice(h * rows + q * rq, h * rows + (q + 1) * rq)
            t = total[h * rq : (h + 1) * rq] * wide(down_c[here, :], L)
            out_ref[here, :] = (keep[here, :].astype(F32) + t).astype(BF)

    for n in range(n_blocks // C):
        with jax.named_scope("settle%d" % n):
            settle(n)
            if n == 0:
                for w in range(1 + U // 2, DOWN):
                    relay(w)
    with jax.named_scope("finish1"):
        for w in range(1, 1 + U):
            finish(w)
    with jax.named_scope("expand"):
        for n in range(n_blocks // C):
            settled(n)
        relay(DOWN)
        lax.fori_loop(0, n_blocks, expand, 0)
    for n in range(Q + 2):
        with jax.named_scope("down%d" % n):
            if n < Q:
                if n + 1 < Q:
                    with jax.named_scope("drel"):
                        relay(DOWN + n + 1)
                with jax.named_scope("dfin"):
                    finish(DOWN + n)
                with jax.named_scope("shrink"):
                    shrink(n)
            if 1 <= n <= Q:
                with jax.named_scope("rcore"):
                    reduce_core(n - 1)
            if n == 2:
                with jax.named_scope("keep"):
                    mine_at = rows_of(tp, width)
                    v = nn(out_full[mine_at, :], mix_g[:, seq_at(g)]) * wide(out_c[mine_at, :], L)
                    keep[...] = (tok_g[mine_at, seq_at(g)].astype(F32) + v).astype(BF)
            if n >= 2:
                with jax.named_scope("ry"):
                    reduce_y(n - 2)
    with jax.named_scope("final"):
        for q in range(Q):
            reduce_z(q)
    for copy, when in pending:
        if when is None:
            copy.wait_send()
        else:
            pl.when(when)(copy.wait_send)

    others = scale_g.at[pl.ds(0, n_dev - 1)]
    remote(others, others, sc_s.at[0], sc_r.at[0], peer(1)).wait_send()
    for w in range(DOWN + Q):
        remote(from_x(w), from_x(w), wxs.at[w], wxr.at[w], to_x(1)).wait_send()


def tables(length, head):
    half = head // 2
    inverse = 1.0 / 10000.0 ** np.linspace(0.0, 1.0, half)
    angle = np.arange(length)[:, None] * inverse.astype(np.float32).astype(np.float64)[None, :]
    spread = lambda a: np.repeat(a, 2, axis=1).T.astype(np.float32)
    return spread(np.cos(angle)), spread(np.sin(angle))


def solution(mesh):
    n_fs, n_tp = mesh.shape["fs"], mesh.shape["tp"]
    heights = [getattr(d, "coords", (0, 0, i))[2] for i, d in enumerate(mesh.devices[:, 0])]
    X = heights.count(heights[0])
    if n_fs % X:
        X = 1
    Z = n_fs // X
    cores = [getattr(d, "core_on_chip", 0) for d in mesh.devices[0]]
    C = len(set(cores))
    if n_tp % C:
        C = 1
    Y = n_tp // C

    def on_device(tokens, mix_gain, mlp_gain, wq, wk, wv, wg, wo, wu, wd, sq, sk, sv, sg, so, su, sd, forget):
        cfg = Cfg()
        cfg.Z, cfg.X, cfg.Y, cfg.C = Z, X, Y, C
        width, L = tokens.shape
        cfg.width, cfg.L, cfg.D = width, L, width * n_tp
        D = cfg.D
        heads = forget.shape[0]
        G = cfg.G = next(q for q in (4, 2, 1) if Z % q == 0 and heads % q == 0)
        ret = cfg.ret = wq.shape[1]
        cfg.head = ret // heads
        hw = cfg.hw = ret // G
        chunk = cfg.chunk = wu.shape[1] // G
        rows = cfg.rows = wq.shape[0]
        n_dev = n_fs * n_tp
        Q = cfg.Q = next(q for q in (8, 4, 2, 1) if rows % (q * 16) == 0)
        U = cfg.U = 2
        scales = [scale_rows(s) for s in (sq, sk, sv, sg, so, sd, su)]
        n_rows = -(-sum(s.shape[0] for s in scales) // 8) * 8
        gains = [v.reshape(-1, LANES) for v in (mix_gain, mlp_gain)]
        cos_t, sin_t = tables(L, cfg.head)
        vm = pl.BlockSpec(memory_space=pltpu.VMEM)
        hbm = pl.BlockSpec(memory_space=pl.ANY)
        dma = pltpu.SemaphoreType.DMA
        strided = rows % LANES == 0
        vmem = lambda *shape, t=BF: pltpu.VMEM(shape, t)
        stack = (lambda *n: vmem(*n, D)) if strided else (lambda *n: vmem(*n[:-1], n_fs, n[-1], rows))
        wt = width // Q
        tb = cfg.tb = 256 if G * L % (256 * C) == 0 else LANES
        scratch = [
            vmem(D, G * L), vmem(ret * n_tp, G * L), vmem(D, ret * n_tp), stack(4 * hw), stack(U, chunk // U),
            vmem(Q, D // Q, chunk), vmem(G, 4 * hw, rows), vmem(G, U, chunk // U, rows), vmem(G, Q, rows // Q, chunk),
            vmem(rows, ret),
            vmem(4, rows, ret, t=F32), vmem(*wo.shape, t=F32), vmem(*wu.shape, t=F32), vmem(*wd.shape, t=F32),
            vmem(Q, D // Q, G * L), vmem(Q, max(C - 1, 1), Y, wt, G * L), vmem(Q, Y, wt, G * L),
            vmem(Q, max(Y - 1, 1), wt, G * L), vmem(Q, wt, G * L), vmem(Q, G, wt, L),
            vmem(G * L // tb, D, tb), vmem(D, L), vmem(chunk, G * L), vmem(width, L),
            vmem(2, D, LANES, t=F32), vmem(D, LANES, t=F32), vmem(G * chunk, LANES, t=F32),
            vmem(width, LANES, t=F32), vmem(4, ret, LANES, t=F32), vmem(hw // cfg.head, L, L, t=F32),
            vmem(n_dev, n_rows, LANES, t=F32), dma((8,)), dma((2 + U + Q,)),
        ]
        y1, c1, x1 = max(Y - 1, 1), max(C - 1, 1), max(X - 1, 1)
        line = lambda n, nx: [(n + 1,), (n,), (n, y1), (n, y1), (n, Y, nx, c1), (n, Y, nx, c1)]
        W = 1 + U + Q
        shapes = [(1,), (1,), (W, max(Z - 1, 1)), (W, max(Z - 1, 1)), (W,), (W,)] + line(G, 1) + line(G, 1)
        first = line(Z, X)
        shapes += first[:4] + [(Z, Y, x1), (Z, Y, x1)] + first[4:]
        shapes += [(Q, c1, Y), (Q, c1, Y), (Q, y1), (Q, y1), (Q, G), (Q, G)]
        shapes += [(G * L // tb // C, c1), (G * L // tb // C, c1)]
        scratch += [dma(s) for s in shapes] + [vmem(n_rows, LANES, t=F32)]
        return pl.pallas_call(
            functools.partial(kernel, cfg),
            out_shape=jax.ShapeDtypeStruct((width, L), BF),
            in_specs=[hbm] + [vm] * 4 + [pl.BlockSpec(memory_space=pltpu.SMEM)] + [hbm] * 7 + [vm] * 7,
            out_specs=vm,
            scratch_shapes=scratch,
            compiler_params=pltpu.CompilerParams(
                collective_id=0, has_side_effects=True, vmem_limit_bytes=63 * 2**20
            ),
            name="layer",
        )(tokens, *gains, jnp.asarray(cos_t), jnp.asarray(sin_t), forget, wq, wk, wv, wg, wo, wu, wd, *scales)

    cut = P(("tp", "fs"))
    rows, cols = P("fs", "tp"), P("tp", "fs")
    in_specs = (cols, P(), P(), rows, rows, rows, rows, cols, rows, cols) + (cut,) * 7 + (P("tp"),)
    return jax.shard_map(on_device, mesh=mesh, in_specs=in_specs, out_specs=cols, check_vma=False)
```

```python
import functools
import math

import jax
import jax.numpy as jnp
import numpy as np
from jax import lax
from jax.experimental import pallas as pl
from jax.experimental.pallas import tpu as pltpu
from jax.sharding import PartitionSpec as P

MESH = pl.DeviceIdType.MESH
BF = jnp.bfloat16
F32 = jnp.float32
LANES = 128


def nn(a, b):
    return lax.dot_general(a, b, (((1,), (0,)), ((), ())), preferred_element_type=F32)


def pick(table, at):
    value = jnp.int32(table[0])
    for a in range(1, len(table)):
        value = jnp.where(at == a, jnp.int32(table[a]), value)
    return value


def part_of(n):
    return min(n, LANES)


def scale_rows(s):
    n = s.shape[0]
    return s.reshape(-1, part_of(n))


class Cfg:
    pass


def kernel(cfg, *refs):
    Z, X, Y, C, G = cfg.Z, cfg.X, cfg.Y, cfg.C, cfg.G
    n_tp, n_fs = Y * C, Z * X
    n_dev = n_tp * n_fs
    L, width, D, ret, hw, chunk, rows = cfg.L, cfg.width, cfg.D, cfg.ret, cfg.hw, cfg.chunk, cfg.rows
    head, Q, U = cfg.head, cfg.Q, cfg.U
    rq, uh = rows // Q, chunk // U
    DOWN = 1 + U
    (tokens, mix_gain, mlp_gain, cos_t, sin_t, forget, wq, wk, wv, wg, wo, wu, wd) = refs[:13]
    own_scales, out_ref = refs[13:20], refs[20]
    (tok_g, mix_g, out_full, f_proj, f_up, f_down, o_proj, o_up, o_down, o_out, st_proj, st_out, st_up, st_down,
     parts, core_in, y_out, y_in, z_out, z_in, after, normed, hidden, keep, gain_c, out_c, up_c, down_c, proj_c,
     decay, scale_g, load_sem, local_sem, sc_s, sc_r, wzs, wzr, wxs, wxr,
     t_zs, t_zr, t_ys, t_yr, t_cs, t_cr, m_zs, m_zr, m_ys, m_yr, m_cs, m_cr,
     p_zs, p_zr, p_ys, p_yr, p_xs, p_xr, p_cs, p_cr, rcs, rcr, rys, ryr, rzs, rzr, ncs, ncr, scales) = refs[21:]
    me = lax.axis_index("fs")
    tp = lax.axis_index("tp")
    z = me // X
    x = lax.rem(me, X)
    y = tp // C
    core = lax.rem(tp, C)
    flat = tp * n_fs + me
    g = lax.rem(z, G)
    base = z - g
    strided = rows % LANES == 0

    def to_z(zz):
        return {"fs": zz * X + x}

    def to_x(o):
        return {"fs": z * X + lax.rem(x + o, X)}

    def to_y(o):
        return {"tp": lax.rem(y + o, Y) * C + core}

    def to_core(o):
        return {"tp": y * C + lax.rem(core + o, C)}

    def peer(o):
        q = lax.rem(flat + o, n_dev)
        return {"fs": lax.rem(q, n_fs), "tp": q // n_fs}

    barrier = pltpu.get_barrier_semaphore()

    def greet(o, carry):
        pl.semaphore_signal(barrier, inc=1, device_id=peer(o), device_id_type=MESH)
        return carry

    lax.fori_loop(1, n_dev, greet, 0)

    def rows_of(i, n):
        return pl.ds(pl.multiple_of(i * n, n), n)

    def seq_at(s):
        return pl.ds(pl.multiple_of(s * L, LANES), L)

    own_tok = tok_g.at[rows_of(tp, width), seq_at(g)]
    loads = [(tokens, own_tok)]
    loads += [(w, st_proj.at[i]) for i, w in enumerate((wq, wk, wv, wg))]
    loads += [(wo, st_out), (wu, st_up), (wd, st_down)]
    loads = [pltpu.make_async_copy(a, b, load_sem.at[i]) for i, (a, b) in enumerate(loads)]
    for copy in loads:
        copy.start()

    pending = []

    def remote(src, dst, ss, rs, where):
        return pltpu.make_async_remote_copy(
            src_ref=src, dst_ref=dst, send_sem=ss, recv_sem=rs, device_id=where, device_id_type=MESH
        )

    pooled = []

    def emit(waits, copies, when=None, track=True):
        def go():
            for copy in waits:
                copy.wait_recv()
            for copy, ok in copies:
                if ok is None:
                    copy.start()
                else:
                    pl.when(ok)(copy.start)

        if when is None:
            go()
        else:
            pl.when(when)(go)
        if track:
            pending.extend(c for c in copies if not any(c[0] is q for q in pooled))

    def begin(*a):
        remote(*a).start()

    def send(*a):
        emit([], [(remote(*a), None)])

    def arrived(ref, ss, rs):
        remote(ref, ref, ss, rs, to_core(1) if C > 1 else to_z(z)).wait_recv()

    class Spread:
        def __init__(self, n, at, first, ref, zs, zr, ys, yr, cs, cr, xs=None, xr=None, pool=None):
            self.pool = pool
            self.n, self.at, self.first, self.ref = n, at, first, ref
            self.zs, self.zr, self.ys, self.yr, self.cs, self.cr, self.xs, self.xr = zs, zr, ys, yr, cs, cr, xs, xr
            self.nx = X if xs is not None else 1

        def order(self, i):
            n = self.n
            return pick([sorted(range(n), key=lambda q: (abs(q - a), q))[i] for a in range(n)], self.at)

        def block(self, i, j, k, o):
            tps = lax.rem(y + Y - j, Y) * C + lax.rem(core + C - o, C)
            return self.ref(self.order(i), lax.rem(x + X - k, X), tps)

        def fan_y(self, i):
            piece = self.block(i, 0, 0, 0)
            return [(remote(piece, piece, self.ys.at[i, j - 1], self.yr.at[i, j - 1], to_y(j)), None)
                    for j in range(1, Y)]

        def fan_x(self, i, j):
            piece = self.block(i, j, 0, 0)
            return [(remote(piece, piece, self.xs.at[i, j, k - 1], self.xr.at[i, j, k - 1], to_x(k)), None)
                    for k in range(1, self.nx)]

        def fan_c(self, i, j, k):
            piece = self.block(i, j, k, 0)
            if self.pool is not None:
                copies = [remote(piece, piece, self.cs.at[0], self.cr.at[0], to_core(o)) for o in range(1, C)]
                pooled.extend(copies)
                return [(copy, None) for copy in copies]
            return [(remote(piece, piece, self.cs.at[i, j, k, o - 1], self.cr.at[i, j, k, o - 1], to_core(o)), None)
                    for o in range(1, C)]

        def fan(self, i):
            return self.fan_y(i) + self.fan_x(i, 0) + self.fan_c(i, 0, 0)

        def start_z(self, when=None, track=True):
            piece = self.block(0, 0, 0, 0)
            slot = self.zr.at[self.at]
            copies = []
            for sem, step in ((0, 1), (self.n, -1)):
                to = self.at + step
                copies.append((remote(piece, piece, self.zs.at[sem], slot, to_z(self.first + to)),
                               (to >= 0) & (to < self.n)))
            emit([], copies, when, track)

        def start(self):
            self.start_z()
            emit([], self.fan(0))

        def on_z(self, i, when=None, track=True):
            o = self.order(i)
            piece = self.block(i, 0, 0, 0)
            nxt = jnp.where(o < self.at, self.at + 1, self.at - 1)
            copy = remote(piece, piece, self.zs.at[i], self.zr.at[o], to_z(self.first + nxt))
            emit([copy], [(copy, (nxt >= 0) & (nxt < self.n))] + self.fan(i), when, track)

        def on_y(self, i, when=None, track=True):
            for j in range(1, Y):
                piece = self.block(i, j, 0, 0)
                wait = remote(piece, piece, self.ys.at[i, j - 1], self.yr.at[i, j - 1], to_y(j))
                emit([wait], self.fan_x(i, j) + self.fan_c(i, j, 0), when, track)

        def on_x(self, i):
            for j in range(Y):
                for k in range(1, self.nx):
                    arrived(self.block(i, j, k, 0), self.xs.at[i, j, k - 1], self.xr.at[i, j, k - 1])
                    emit([], self.fan_c(i, j, k))

        def all_c(self):
            if C > 1:
                arrived(self.pool, self.cs.at[0], self.cr.at[0])
                pending.append((remote(self.pool, self.pool, self.cs.at[0], self.cr.at[0], to_core(1)), None))

        def on_c(self, i):
            for j in range(Y):
                for k in range(self.nx):
                    for o in range(1, C):
                        arrived(self.block(i, j, k, o), self.cs.at[i, j, k, o - 1], self.cr.at[i, j, k, o - 1])

    tok = Spread(G, g, base, lambda zi, xi, t: tok_g.at[rows_of(t, width), seq_at(zi)], t_zs, t_zr, t_ys, t_yr, t_cs, t_cr)
    mix = Spread(G, g, base, lambda zi, xi, t: mix_g.at[pl.ds(pl.multiple_of(t * ret + zi * hw, hw), hw)],
                 m_zs, m_zr, m_ys, m_yr, m_cs, m_cr, pool=mix_g.at[pl.ds(0, ret * Y * (C - 1))])
    prj = Spread(Z, z, 0, lambda zi, xi, t: out_full.at[rows_of(zi * X + xi, rows), rows_of(t, ret)],
                 p_zs, p_zr, p_ys, p_yr, p_cs, p_cr, p_xs, p_xr, pool=out_full.at[pl.ds(0, D // C * (C - 1))])

    def place(w, owner):
        if w >= DOWN:
            return f_down.at[w - DOWN, rows_of(owner, rq)]
        ref = f_proj if w == 0 else f_up.at[w - 1]
        return ref.at[:, rows_of(owner, rows)] if strided else ref.at[owner]

    def mine(w, k):
        if w >= DOWN:
            return o_down.at[k, w - DOWN]
        return o_proj.at[k] if w == 0 else o_up.at[k, w - 1]

    def mul(ref, v):
        if strided:
            return nn(ref[...], v)
        total = nn(ref[0], v[0:rows, :])
        for f in range(1, n_fs):
            total += nn(ref[f], v[f * rows : (f + 1) * rows, :])
        return total

    locals_ = {}

    def z_send(w, when=None, track=True, ends_too=None):
        copies = []
        for i in range(1, Z):
            to = prj.order(i)
            o = lax.rem(to + Z - z, Z) - 1
            copy = remote(mine(w, lax.rem(to, G)), place(w, me), wzs.at[w], wzr.at[w, o], to_z(to))
            ok = None
            if ends_too is not None:
                ok = (to == 0) | (to == Z - 1)
                ok = ok if ends_too else jnp.logical_not(ok)
            copies.append((copy, ok))
        emit([], copies, when, False)

    def from_x(w, n=Z * (X - 1)):
        if w >= DOWN:
            return f_down.at[w - DOWN, pl.ds(0, n * rq)]
        ref = f_proj if w == 0 else f_up.at[w - 1]
        return ref.at[:, pl.ds(0, n * rows)] if strided else ref.at[pl.ds(0, n)]

    def x_own(w):
        for o in range(1, X):
            remote(mine(w, g), place(w, me), wxs.at[w], wxr.at[w], to_x(o)).start()
        copy = pltpu.make_async_copy(mine(w, g), place(w, me), local_sem.at[w])
        copy.start()
        locals_[w] = copy

    def relay(w, when=None, track=True):
        for k in range(1, Z):
            piece = place(w, lax.rem(z + Z - k, Z) * X + x)
            wait = remote(piece, piece, wzs.at[w], wzr.at[w, k - 1], to_x(1) if X > 1 else to_core(1))
            emit([wait], [(remote(piece, piece, wxs.at[w], wxr.at[w], to_x(o)), None) for o in range(1, X)],
                 when, False)

    def finish(w):
        locals_[w].wait()
        arrived(from_x(w), wxs.at[w], wxr.at[w])

    def wide(col, n):
        return jnp.concatenate([col] * (n // LANES), axis=1) if n > LANES else col[:, :n]

    def column(row):
        return jnp.broadcast_to(row, (LANES, LANES)).T

    def columns(dst, row, n, count, first):
        w = part_of(n)
        per = n // w

        def one(f, carry):
            for r in range(per):
                c = column(scale_g[first + f, row + r : row + r + 1, :])[:w]
                if w % 8 == 0:
                    dst[pl.ds(pl.multiple_of((f * per + r) * w, 8), w), :] = c
                else:
                    dst[f * w : (f + 1) * w, :] = c
            return carry

        if w % 8 == 0:
            lax.fori_loop(0, count, one, 0, unroll=math.gcd(count, 4))
        else:
            for f in range(count):
                one(f, 0)

    loads[0].wait()
    scales[...] = jnp.zeros_like(scales)
    at = 0
    for ref in own_scales:
        n, w = ref.shape
        scales[at : at + n, :w] = ref[...]
        at += n
    scale_g[flat] = scales[...]
    pl.semaphore_wait(barrier, n_dev - 1)

    with jax.named_scope("start"):
        tok.start()

        def tell(o, carry):
            remote(scales, scale_g.at[flat], sc_s.at[0], sc_r.at[0], peer(o)).start()
            return carry

        lax.fori_loop(1, n_dev, tell, 0)

    ends = (z == 0) | (z == Z - 1)
    with jax.named_scope("cast"):
        for i in range(4):
            loads[1 + i].wait()
            t = st_proj[i].T
            for k in range(G):
                o_proj[k, i * hw : (i + 1) * hw, :] = t[k * hw : (k + 1) * hw, :].astype(BF)
        z_send(0, when=ends)
        x_own(0)
        loads[5].wait()
        own_out = out_full.at[rows_of(me, rows), rows_of(tp, ret)]
        o_out[...] = st_out[...].T.astype(BF)
        copy = pltpu.make_async_copy(o_out, own_out, local_sem.at[DOWN + Q])
        copy.start()
        copy.wait()
        prj.start_z(ends)
        loads[6].wait()
        loads[7].wait()

        def cast_up(k, carry):
            at = rows_of(k, chunk)
            t = st_up[:, at].T.astype(BF)
            for i in range(U):
                o_up[k, i] = t[i * uh : (i + 1) * uh]
            t = st_down[at, :].T.astype(BF)
            for i in range(Q):
                o_down[k, i] = t[i * rq : (i + 1) * rq]
            return carry

        lax.fori_loop(0, G, cast_up, 0)
        for w in range(1, DOWN + Q):
            x_own(w)

    with jax.named_scope("tables"):
        def gain_row(i, carry):
            gain_c[0, rows_of(i, LANES), :] = column(mix_gain[pl.ds(i, 1), :])
            gain_c[1, rows_of(i, LANES), :] = column(mlp_gain[pl.ds(i, 1), :])
            return carry

        lax.fori_loop(0, D // LANES, gain_row, 0, unroll=4)
        krow = lax.broadcasted_iota(jnp.int32, (L, L), 0)
        qcol = lax.broadcasted_iota(jnp.int32, (L, L), 1)
        dist = (qcol - krow).astype(F32)
        for h in range(hw // head):
            rate = forget[g * (hw // head) + h]
            decay[h] = jnp.where(dist >= 0.0, jnp.exp(-rate * jnp.maximum(dist, 0.0)), 0.0)

    with jax.named_scope("tok1"):
        tok.on_z(1)
        if G > 2:
            tok.on_z(2)
        z_send(0, when=jnp.logical_not(ends), track=False)
        tok.on_y(0)
    with jax.named_scope("scales"):
        others = scale_g.at[pl.ds(0, n_dev - 1)]
        arrived(others, sc_s.at[0], sc_r.at[0])
        for i in range(4):
            columns(proj_c.at[i], i, ret // n_fs, n_fs, tp * n_fs)
    with jax.named_scope("columns"):
        columns(out_c, 4, D // n_dev, n_dev, 0)
        columns(down_c, 5, width // n_fs, n_fs, tp * n_fs)
        columns(up_c, 6, G * chunk // n_fs, n_fs, tp * n_fs)
    inner = jnp.logical_not(ends)
    with jax.named_scope("tok_y1"):
        tok.on_y(1)
    with jax.named_scope("relay0"):
        relay(0, when=ends)
        for w in range(1, DOWN):
            z_send(w, when=ends)
    with jax.named_scope("tok3"):
        for i in range(3, G):
            tok.on_z(i)
    with jax.named_scope("relay0b"):
        prj.start_z(inner, track=False)
        emit([], prj.fan(0))
        relay(0, when=inner, track=False)
        for k in range(1, min(Z, 3)):
            prj.on_z(k, when=inner)
    with jax.named_scope("finish0"):
        finish(0)

    tile = 256 if D % 256 == 0 else D
    r64 = lax.broadcasted_iota(jnp.int32, (head, head), 0)
    c64 = lax.broadcasted_iota(jnp.int32, (head, head), 1)
    odd = lax.rem(r64, 2) == 1
    swap = jnp.where((c64 == r64 - 1) & odd, 1.0, jnp.where((c64 == r64 + 1) & ~odd, -1.0, 0.0)).astype(BF)

    def turn(field):
        return field.astype(F32) * cos_t[...] + nn(swap, field) * sin_t[...]

    def attend(i):
        at = seq_at(tok.order(i))

        def add(t, square):
            v = tok_g[rows_of(t, tile), at].astype(F32)
            return square + jnp.sum(v * v, axis=0, keepdims=True)

        square = lax.fori_loop(0, D // tile, add, jnp.zeros((1, L), F32))
        factor = lax.rsqrt(square / D + 1e-6)

        def one(t, carry):
            here = rows_of(t, tile)
            normed[here, :] = (tok_g[here, at].astype(F32) * factor * wide(gain_c[0, here, :], L)).astype(BF)
            return carry

        lax.fori_loop(0, D // tile, one, 0)
        proj = mul(f_proj, normed[...])
        heads_at = pl.ds(pl.multiple_of(g * hw, hw), hw)
        q, k, v, gate = [
            (proj[n * hw : (n + 1) * hw, :] * wide(proj_c[n, heads_at, :], L)).astype(BF) for n in range(4)
        ]
        for h in range(hw // head):
            of = slice(h * head, (h + 1) * head)
            rot_q = turn(q[of]).astype(BF)
            rot_k = (turn(k[of]) * head ** (-0.5)).T.astype(BF)
            inner = (nn(rot_k, rot_q) * decay[h]).astype(BF)
            total = nn(v[of], inner)
            mean = jnp.sum(total * total, axis=0, keepdims=True) / head
            f = gate[of].astype(F32)
            value = f / (1.0 + jnp.exp(-f)) * (total * lax.rsqrt(mean + 0.01))
            mix_g[pl.ds(pl.multiple_of(tp * ret + g * hw + h * head, head), head), at] = value.astype(BF)

    with jax.named_scope("tok_y2"):
        for i in range(2, G - 1):
            tok.on_y(i)
    for i in range(G):
        if i == G - 1 and i > 1:
            with jax.named_scope("tok_y3"):
                tok.on_y(i, when=ends, track=False)
        with jax.named_scope("att%d" % i):
            tok.on_c(i)
            attend(i)
        if i == 0 and G > 2:
            with jax.named_scope("tok_y3"):
                tok.on_y(G - 1, when=inner)
        if i == min(1, G - 1):
            with jax.named_scope("prj_z0"):
                for k in range(3, Z):
                    prj.on_z(k, when=inner)
                for w in range(1, 1 + U // 2):
                    z_send(w, when=inner, track=False)
        if i == G - 2:
            with jax.named_scope("prj_y0"):
                prj.on_y(0)
    with jax.named_scope("mix_start"):
        mix.start()
    with jax.named_scope("prj_y12"):
        for k in range(1, min(Z, 3)):
            prj.on_y(k, when=inner)
    with jax.named_scope("prj_z"):
        for k in range(1, min(Z, 3)):
            prj.on_z(k, when=ends, track=False)
        for k in range(3, Z):
            prj.on_z(k, when=ends, track=False)
    with jax.named_scope("mix_z"):
        for i in range(1, min(G, 3)):
            mix.on_z(i)
    with jax.named_scope("prj_y1"):
        for k in range(1, min(Z, 3)):
            prj.on_y(k, when=ends, track=False)
    with jax.named_scope("mix_z3"):
        for i in range(3, G):
            mix.on_z(i)
    for w in range(DOWN, DOWN + Q):
        z_send(w, when=ends)
    with jax.named_scope("prj_y3"):
        for k in range(3, Z):
            prj.on_y(k)
    with jax.named_scope("relay1"):
        for w in range(1, 1 + U // 2):
            relay(w)
    with jax.named_scope("mix_y"):
        for i in range(G):
            mix.on_y(i)
            if i == 1:
                for w in range(1 + U // 2, DOWN + Q):
                    z_send(w, when=inner, track=False)
    with jax.named_scope("prj_x"):
        for k in range(Z):
            prj.on_x(k)
    with jax.named_scope("prj_c"):
        prj.all_c()
    with jax.named_scope("mix_c"):
        mix.all_c()

    tb = cfg.tb
    n_blocks = G * L // tb

    def settle(n):
        b = n * C + core
        at = rows_of(b, tb)
        v = nn(out_full[...], mix_g[:, at]) * wide(out_c[...], tb)
        a = (tok_g[:, at].astype(F32) + v).astype(BF).astype(F32)
        factor = lax.rsqrt(jnp.sum(a * a, axis=0, keepdims=True) / D + 1e-6)
        after[b] = (a * factor * wide(gain_c[1], tb)).astype(BF)
        for o in range(1, C):
            send(after.at[b], after.at[b], ncs.at[n, o - 1], ncr.at[n, o - 1], to_core(o))

    def settled(n):
        for o in range(1, C):
            arrived(after.at[n * C + lax.rem(core + C - o, C)], ncs.at[n, o - 1], ncr.at[n, o - 1])

    def expand(i, b, carry):
        at = rows_of(b, tb)
        if i < U:
            sc = wide(up_c[pl.ds(pl.multiple_of(g * chunk + i * uh, uh), uh), :], tb)
            u = jnp.maximum(mul(f_up.at[i], after[b]) * sc, 0.0)
            hidden[i * uh : (i + 1) * uh, at] = (u * u).astype(BF)
        return carry

    wt = width // Q
    ppt = n_fs // n_tp

    def shrink(q):
        def one(b, carry):
            at = rows_of(b, tb)
            parts[q, :, at] = nn(f_down[q], hidden[:, at]).astype(BF)
            return carry

        lax.fori_loop(0, G * L // tb, one, 0)
        for o in range(1, C):
            for j in range(Y):
                begin(parts.at[q, rows_of(j * C + lax.rem(core + o, C), wt)], core_in.at[q, o - 1, j],
                     rcs.at[q, o - 1], rcr.at[q, o - 1], to_core(o))

    def reduce_core(q):
        for o in range(1, C):
            arrived(core_in.at[q, o - 1], rcs.at[q, o - 1], rcr.at[q, o - 1])
            pending.append((remote(core_in.at[q, o - 1], core_in.at[q, o - 1], rcs.at[q, o - 1], rcr.at[q, o - 1],
                                   to_core(o)), None))
        for n in range(Y - 1, -1, -1):
            j = lax.rem(y + n, Y)
            value = parts[q, rows_of(j * C + core, wt), :].astype(F32)
            for o in range(1, C):
                value += core_in[q, o - 1, j].astype(F32)
            y_out[q, j] = value.astype(BF)
            if n:
                send(y_out.at[q, j], y_in.at[q, n - 1], rys.at[q, n - 1], ryr.at[q, n - 1], to_y(n))

    def reduce_y(q):
        value = y_out[q, y].astype(F32)
        for j in range(1, Y):
            arrived(y_in.at[q, j - 1], rys.at[q, j - 1], ryr.at[q, j - 1])
            value += y_in[q, j - 1].astype(F32)
        z_out[q] = value.astype(BF)
        for i in range(G - 1, 0, -1):
            s = tok.order(i)
            slot = z_in.at[q, lax.rem(g + G - s, G) - 1]
            begin(z_out.at[q, :, seq_at(s)], slot, rzs.at[q], rzr.at[q], to_z(base + s))

    def reduce_z(q):
        total = z_out[q, :, seq_at(g)].astype(F32)
        if G > 1:
            arrived(z_in.at[q], rzs.at[q], rzr.at[q])
            pending.append((remote(z_in.at[q], z_in.at[q], rzs.at[q], rzr.at[q], to_z(base)), None))
        for i in range(G - 1):
            total += z_in[q, i].astype(F32)
        for h in range(ppt):
            here = slice(h * rows + q * rq, h * rows + (q + 1) * rq)
            t = total[h * rq : (h + 1) * rq] * wide(down_c[here, :], L)
            out_ref[here, :] = (keep[here, :].astype(F32) + t).astype(BF)

    for n in range(n_blocks // C):
        with jax.named_scope("settle%d" % n):
            settle(n)
            if n == 0:
                for w in range(1 + U // 2, DOWN):
                    relay(w)
    with jax.named_scope("finish1"):
        finish(1)
    with jax.named_scope("expand"):
        for n in range(n_blocks // C):
            settled(n)
        for i in range(U):
            if i:
                with jax.named_scope("finish2"):
                    finish(1 + i)
                relay(DOWN)
            lax.fori_loop(0, n_blocks, functools.partial(expand, i), 0)
        relay(DOWN + 1)
    for n in range(Q + 2):
        with jax.named_scope("down%d" % n):
            if n < Q:
                with jax.named_scope("dfin"):
                    finish(DOWN + n)
                with jax.named_scope("shrink"):
                    shrink(n)
                with jax.named_scope("rcore"):
                    reduce_core(n)
                if n + 2 < Q:
                    with jax.named_scope("drel"):
                        relay(DOWN + n + 2)
            if n == 1:
                with jax.named_scope("keep"):
                    mine_at = rows_of(tp, width)
                    v = nn(out_full[mine_at, :], mix_g[:, seq_at(g)]) * wide(out_c[mine_at, :], L)
                    keep[...] = (tok_g[mine_at, seq_at(g)].astype(F32) + v).astype(BF)
            if n >= 2:
                with jax.named_scope("ry"):
                    reduce_y(n - 2)
    with jax.named_scope("final"):
        for q in range(Q):
            reduce_z(q)
    for copy, when in pending:
        if when is None:
            copy.wait_send()
        else:
            pl.when(when)(copy.wait_send)

    others = scale_g.at[pl.ds(0, n_dev - 1)]
    remote(others, others, sc_s.at[0], sc_r.at[0], peer(1)).wait_send()
    for w in range(DOWN + Q):
        remote(from_x(w), from_x(w), wxs.at[w], wxr.at[w], to_x(1)).wait_send()
        remote(from_x(w, Z - 1), from_x(w, Z - 1), wzs.at[w], wxr.at[w], to_x(1)).wait_send()


def tables(length, head):
    half = head // 2
    inverse = 1.0 / 10000.0 ** np.linspace(0.0, 1.0, half)
    angle = np.arange(length)[:, None] * inverse.astype(np.float32).astype(np.float64)[None, :]
    spread = lambda a: np.repeat(a, 2, axis=1).T.astype(np.float32)
    return spread(np.cos(angle)), spread(np.sin(angle))


def solution(mesh):
    n_fs, n_tp = mesh.shape["fs"], mesh.shape["tp"]
    heights = [getattr(d, "coords", (0, 0, i))[2] for i, d in enumerate(mesh.devices[:, 0])]
    X = heights.count(heights[0])
    if n_fs % X:
        X = 1
    Z = n_fs // X
    cores = [getattr(d, "core_on_chip", 0) for d in mesh.devices[0]]
    C = len(set(cores))
    if n_tp % C:
        C = 1
    Y = n_tp // C

    def on_device(tokens, mix_gain, mlp_gain, wq, wk, wv, wg, wo, wu, wd, sq, sk, sv, sg, so, su, sd, forget):
        cfg = Cfg()
        cfg.Z, cfg.X, cfg.Y, cfg.C = Z, X, Y, C
        width, L = tokens.shape
        cfg.width, cfg.L, cfg.D = width, L, width * n_tp
        D = cfg.D
        heads = forget.shape[0]
        G = cfg.G = next(q for q in (4, 2, 1) if Z % q == 0 and heads % q == 0)
        ret = cfg.ret = wq.shape[1]
        cfg.head = ret // heads
        hw = cfg.hw = ret // G
        chunk = cfg.chunk = wu.shape[1] // G
        rows = cfg.rows = wq.shape[0]
        n_dev = n_fs * n_tp
        Q = cfg.Q = next(q for q in (8, 4, 2, 1) if rows % (q * 16) == 0)
        U = cfg.U = 2
        scales = [scale_rows(s) for s in (sq, sk, sv, sg, so, sd, su)]
        n_rows = -(-sum(s.shape[0] for s in scales) // 8) * 8
        gains = [v.reshape(-1, LANES) for v in (mix_gain, mlp_gain)]
        cos_t, sin_t = tables(L, cfg.head)
        vm = pl.BlockSpec(memory_space=pltpu.VMEM)
        hbm = pl.BlockSpec(memory_space=pl.ANY)
        dma = pltpu.SemaphoreType.DMA
        strided = rows % LANES == 0
        vmem = lambda *shape, t=BF: pltpu.VMEM(shape, t)
        stack = (lambda *n: vmem(*n, D)) if strided else (lambda *n: vmem(*n[:-1], n_fs, n[-1], rows))
        wt = width // Q
        tb = cfg.tb = 256 if G * L % (256 * C) == 0 else LANES
        scratch = [
            vmem(D, G * L), vmem(ret * n_tp, G * L), vmem(D, ret * n_tp), stack(4 * hw), stack(U, chunk // U),
            vmem(Q, D // Q, chunk), vmem(G, 4 * hw, rows), vmem(G, U, chunk // U, rows), vmem(G, Q, rows // Q, chunk),
            vmem(rows, ret),
            vmem(4, rows, ret, t=F32), vmem(*wo.shape, t=F32), vmem(*wu.shape, t=F32), vmem(*wd.shape, t=F32),
            vmem(Q, D // Q, G * L), vmem(Q, max(C - 1, 1), Y, wt, G * L), vmem(Q, Y, wt, G * L),
            vmem(Q, max(Y - 1, 1), wt, G * L), vmem(Q, wt, G * L), vmem(Q, max(G - 1, 1), wt, L),
            vmem(G * L // tb, D, tb), vmem(D, L), vmem(chunk, G * L), vmem(width, L),
            vmem(2, D, LANES, t=F32), vmem(D, LANES, t=F32), vmem(G * chunk, LANES, t=F32),
            vmem(width, LANES, t=F32), vmem(4, ret, LANES, t=F32), vmem(hw // cfg.head, L, L, t=F32),
            vmem(n_dev, n_rows, LANES, t=F32), dma((8,)), dma((2 + U + Q,)),
        ]
        y1, c1, x1 = max(Y - 1, 1), max(C - 1, 1), max(X - 1, 1)
        line = lambda n, nx: [(n + 1,), (n,), (n, y1), (n, y1), (n, Y, nx, c1), (n, Y, nx, c1)]
        W = 1 + U + Q
        pooled = lambda n, nx: line(n, nx)[:4] + [(1,), (1,)]
        shapes = [(1,), (1,), (W,), (W, max(Z - 1, 1)), (W,), (W,)] + line(G, 1) + pooled(G, 1)
        first = pooled(Z, X)
        shapes += first[:4] + [(Z, Y, x1), (Z, Y, x1)] + first[4:]
        shapes += [(Q, c1), (Q, c1), (Q, y1), (Q, y1), (Q,), (Q,)]
        shapes += [(G * L // tb // C, c1), (G * L // tb // C, c1)]
        scratch += [dma(s) for s in shapes] + [vmem(n_rows, LANES, t=F32)]
        return pl.pallas_call(
            functools.partial(kernel, cfg),
            out_shape=jax.ShapeDtypeStruct((width, L), BF),
            in_specs=[hbm] + [vm] * 4 + [pl.BlockSpec(memory_space=pltpu.SMEM)] + [hbm] * 7 + [vm] * 7,
            out_specs=vm,
            scratch_shapes=scratch,
            compiler_params=pltpu.CompilerParams(
                collective_id=0, has_side_effects=True, vmem_limit_bytes=63 * 2**20
            ),
            name="layer",
        )(tokens, *gains, jnp.asarray(cos_t), jnp.asarray(sin_t), forget, wq, wk, wv, wg, wo, wu, wd, *scales)

    cut = P(("tp", "fs"))
    rows, cols = P("fs", "tp"), P("tp", "fs")
    in_specs = (cols, P(), P(), rows, rows, rows, rows, cols, rows, cols) + (cut,) * 7 + (P("tp"),)
    return jax.shard_map(on_device, mesh=mesh, in_specs=in_specs, out_specs=cols, check_vma=False)
```
